128 devices in a mesh: grp: 4 (over y, x), ep: 32 (over z, core).
Axes of the slice: x: 2, y: 2, z: 16, core: 2. Of those that a mesh axis runs over, the one named last changes fastest.
The devices are a block of a 8x8x16 slice.
Arguments:
- tokens: bfloat16 [2048, 2048], P(('grp', 'ep')), parts along dimension 0, may hold values from -6 to 6
- norm_gain: bfloat16 [2048], replicated, may hold values from 0.099609375 to 1.8984375
- query_weight: bfloat16 [2048, 1024], P(None, 'ep'), may hold values from -0.125 to 0.125
- key_weight: bfloat16 [2048, 256], replicated, may hold values from -0.25 to 0.25
- value_weight: bfloat16 [2048, 256], replicated, may hold values from -0.125 to 0.125
- out_weight: bfloat16 [1024, 2048], P(None, 'ep'), may hold values from -0.1875 to 0.1875
- head_gain: bfloat16 [128], replicated, may hold values from 0.099609375 to 1.8984375
- lambdas: float32 [8], replicated, may hold values from 0.3 to 0.8
- cache_keys: bfloat16 [2048, 1024, 2, 128], P(('grp', 'ep')), parts along dimension 0, may hold values from -1000 to 1000
- cache_values: bfloat16 [2048, 1024, 2, 128], P(('grp', 'ep')), parts along dimension 0, may hold values from -6 to 6
- lengths: int32 [2048], P(('grp', 'ep')), parts along dimension 0, may hold values from 64 to 1024
- moe_gain: bfloat16 [2048], replicated, may hold values from 0.099609375 to 1.8984375
- gate_weight: bfloat16 [32, 2048, 1024], P('ep'), may hold values from -0.375 to 0.375
- up_weight: bfloat16 [32, 2048, 1024], P('ep'), may hold values from -0.375 to 0.375
- down_weight: bfloat16 [32, 1024, 2048], P('ep'), may hold values from -0.02734375 to 0.02734375
- routes: int32 [2048, 4], P(('grp', 'ep')), parts along dimension 0, may hold values from 0 to 31, all different within a row; in each aligned block of 16 rows (0 to 15, 16 to 31, ...) at most 4 rows name the same one
- route_weights: float32 [2048, 4], P(('grp', 'ep')), parts along dimension 0, may hold values from 0.2 to 1
Outputs:
- mixed: bfloat16 [2048, 2048], P(('grp', 'ep')), parts along dimension 0
The draws below stay inside these ranges and needn't reach their ends.
There are 4 independent parts, one for each index of `grp`. The reference program is written for one: setup_inputs(seed, part) draws one part's arguments, and reference() takes and returns one part's arrays. A program takes and returns all parts, laid end to end along the dimension named above; an argument that names none is the same for every part. Nothing has to cross between parts.
Inputs may be any that keep to these rules, and one draw needn't show every extreme that they name: `routes`: a token's 4 experts differ; the tokens of one device name each expert at most 4 times, and in every draw some expert is named exactly 4 times by one device's tokens.
All inputs are finite; a program needn't handle non-finite values.
Results may differ from the reference program's by a relative error of at most 0.034.
Values may be sent and summed in bfloat16 or wider, within the bound.
No kernel may reach another device: no remote copies, remote signals or barrier semaphores. Data moves between devices by JAX's collectives and lax.ppermute only.
A program may use at most 128 MiB of HBM per device.

```python
import math
import jax
import jax.numpy as jnp
import numpy as np
from jax import lax

D = 2048
HEADS = 8
KV_HEADS = 2
DH = 64
VAL = 128
FF = 1024
TOPK = 4
SEQ_DEV = 16
CTX = 1024
EXPERTS = 32
CAP = 4
SEQS = 512
N_EP = 32


def draw_cache_keys(key, part):
    shape = (SEQS, CTX, KV_HEADS, 2 * DH)
    base = jax.random.normal(key, shape, jnp.float32) * 1.75
    return base.astype(jnp.bfloat16)


def plant(entries, stream_key, smallest, largest):
    longest = entries.shape.index(max(entries.shape))
    spots = []
    for shift in (0, 1):
        where = [jax.random.randint(jax.random.fold_in(stream_key, axis), (), 0, length) for axis, length in enumerate(entries.shape)]
        where[longest] = (where[longest] + shift) % entries.shape[longest]
        spots.append(tuple(where))
    return entries.at[spots[0]].set(smallest).at[spots[1]].set(largest)


def shard_levels(key, extent, cuts, low, top_value):
    def one(dim, parts):
        heights = jax.random.uniform(jax.random.fold_in(jax.random.fold_in(key, 6), dim), (parts,), jnp.float32, low / len(cuts), top_value / len(cuts))
        return jnp.repeat(jnp.exp(heights), extent[dim] // parts).reshape((-1,) + (1,) * (len(extent) - dim - 1))

    level = one(*cuts[0])
    for cut in cuts[1:]:
        level = level * one(*cut)
    return level


def shared_out(rng, own, number, rows, amount, top, reach, skew):
    ranking = jax.random.permutation(rng, amount)
    packed, common = portions_of(amount, rows * top, reach, skew, True), portions_of(amount, rows * top, reach, skew, False)
    places = jnp.arange(amount)

    def named(tallies, offset_by):
        used = int((tallies > 0).sum())
        fixed = max(1, used // 4)
        moved = fixed + (places - fixed + offset_by * (used - fixed)) % max(1, amount - fixed)
        return jnp.zeros((amount,), jnp.int32).at[ranking[jnp.where(places < fixed, places, moved)]].set(jnp.asarray(tallies, jnp.int32))

    tallies = jnp.where(number % 4 == 0, named(packed, number // 4), named(common, number - number // 4 - 1))
    mixed = jax.random.permutation(jax.random.fold_in(own, 3), amount)
    donor, taker = mixed[0:amount // 2 * 2:2], mixed[1:amount // 2 * 2:2]
    room = jnp.minimum(tallies[donor] - 1, reach - tallies[taker]) // 2
    room = jnp.where((donor == ranking[0]) | (taker == ranking[0]) | (tallies[taker] == 0), 0, jnp.maximum(room, 0))
    moved = jax.random.randint(jax.random.fold_in(own, 4), (amount // 2,), 0, 1 << 20) % (room + 1)
    tallies = tallies.at[donor].add(-moved).at[taker].add(moved)
    members = jnp.searchsorted(jnp.cumsum(tallies), jnp.arange(rows * top), side="right").astype(jnp.int32)
    listing = members.reshape(top, rows).T
    listing = listing[jax.random.permutation(jax.random.fold_in(own, 1), rows)]
    offset_by = jax.random.randint(jax.random.fold_in(own, 2), (rows, 1), 0, top)
    return jnp.take_along_axis(listing, (jnp.arange(top)[None, :] + offset_by) % top, axis=1)


def portions_of(amount, total, bound, lean, full):
    portions = [(1 << 20) // math.isqrt(standing ** lean) + 1 for standing in range(1, amount + 1)]
    largest = bound if full else min(bound, max(-(-total // amount), total * portions[0] // sum(portions)))
    least = 1 if total - largest >= amount - 1 else 0
    counts, surplus = [largest] + [least] * (amount - 1), total - largest - least * (amount - 1)
    while surplus > 0:
        candidates = [i for i in range(1, amount) if counts[i] < largest] or [i for i in range(1, amount) if counts[i] < bound]
        whole, budget = sum([portions[i] for i in candidates]), surplus
        for i in candidates:
            more = min(bound - counts[i], max(1, budget * portions[i] // whole), surplus)
            counts[i] = counts[i] + more
            surplus = surplus - more
    return np.array(counts)


def centred(rng, shape, scale, most, cuts=(), held_as=jnp.bfloat16):
    drawn = scale * jax.random.normal(rng, shape, jnp.float32)
    if cuts:
        drawn = drawn * shard_levels(rng, shape, cuts, -0.22, 0.18)
    return jnp.clip(drawn, -most, most).astype(held_as)


def setup_inputs(seed: int = 0, part: int = 0) -> dict:
    arg_keys = jax.random.split(jax.random.key(seed), 18)
    part_keys = jax.random.split(jax.random.fold_in(arg_keys[17], part), 18)
    tokens = centred(part_keys[0], (SEQS, D), 1.0, 6.0, ((0, 32),))
    norm_gain = jnp.clip(1.0 + 0.18 * jax.random.normal(arg_keys[1], (D,), jnp.float32), 0.099609375, 1.8984375).astype(jnp.bfloat16)
    query_weight = centred(arg_keys[2], (D, 2 * HEADS * DH), D ** -0.5, 0.125, ((1, 32),))
    key_weight = centred(arg_keys[3], (D, 2 * KV_HEADS * DH), (D // 4) ** -0.5, 0.25)
    value_weight = centred(arg_keys[4], (D, KV_HEADS * VAL), D ** -0.5, 0.125)
    out_weight = centred(arg_keys[5], (HEADS * VAL, D), (HEADS * VAL) ** -0.5, 0.1875, ((1, 32),))
    head_gain = jnp.clip(1.0 + 0.18 * jax.random.normal(arg_keys[6], (VAL,), jnp.float32), 0.099609375, 1.8984375).astype(jnp.bfloat16)
    lambdas = jnp.clip(jax.random.uniform(arg_keys[7], (HEADS,), jnp.float32, 0.3, 0.8), 0.3, 0.8)
    cache_keys = draw_cache_keys(jax.random.fold_in(jax.random.fold_in(arg_keys[17], part), 71), part)
    cache_values = centred(part_keys[9], (SEQS, CTX, KV_HEADS, VAL), 1.0, 6.0, ((0, 32),))
    lengths = plant(jax.random.randint(part_keys[10], (SEQS,), CTX // 16, CTX + 1), jax.random.fold_in(part_keys[10], 1), CTX // 16, CTX).astype(jnp.int32)
    moe_gain = jnp.clip(1.0 + 0.18 * jax.random.normal(arg_keys[11], (D,), jnp.float32), 0.099609375, 1.8984375).astype(jnp.bfloat16)
    gate_weight = centred(arg_keys[12], (EXPERTS, D, FF), (D // 9) ** -0.5, 0.375, ((0, 32),))
    up_weight = centred(arg_keys[13], (EXPERTS, D, FF), (D // 9) ** -0.5, 0.375, ((0, 32),))
    down_weight = centred(arg_keys[14], (EXPERTS, FF, D), (FF * 48) ** -0.5, 0.02734375, ((0, 32),))
    routes_keys = jax.random.split(jax.random.fold_in(part_keys[15], 1), SEQS // SEQ_DEV)
    routes_turns = jax.random.permutation(jax.random.fold_in(part_keys[15], 3), SEQS // SEQ_DEV)
    routes = jax.vmap(lambda own, number: shared_out(jax.random.fold_in(part_keys[15], 2), own, number, SEQ_DEV, EXPERTS, TOPK, CAP, 2))(routes_keys, routes_turns).reshape((SEQS, TOPK))
    route_weights = jnp.clip(0.2 + 0.8 * jax.random.uniform(part_keys[16], (SEQS, TOPK), jnp.float32) ** shard_levels(part_keys[16], (SEQS, TOPK), ((0, 32),), -0.2, 0.2), 0.2, 1.0)
    return dict(tokens=tokens, norm_gain=norm_gain, query_weight=query_weight, key_weight=key_weight, value_weight=value_weight, out_weight=out_weight, head_gain=head_gain, lambdas=lambdas, cache_keys=cache_keys, cache_values=cache_values, lengths=lengths, moe_gain=moe_gain, gate_weight=gate_weight, up_weight=up_weight, down_weight=down_weight, routes=routes, route_weights=route_weights)


epsilon = 1e-06
masked_score = -1e+30
clamp_limit = 7.0
swish_alpha = 1.702

def rms_scaled(values, gain):
    floats = values.astype(jnp.float32)
    return floats * lax.rsqrt(lax.optimization_barrier(jnp.mean(floats * floats, axis=-1, keepdims=True)) + epsilon) * gain.astype(jnp.float32)

def attention(queries, new_keys, new_values, cache_keys, cache_values, lengths, lambdas, head_gain):
    count = queries.shape[0]
    ctx_len = cache_keys.shape[1]
    kv_count = cache_keys.shape[2]
    head_dim = cache_keys.shape[3] // 2
    heads = lambdas.shape[0]
    group = heads // kv_count
    val_dim = cache_values.shape[3]
    query_grid = queries.reshape(count, kv_count, group, 2, head_dim).astype(jnp.float32)
    key_grid = cache_keys.reshape(count, ctx_len, kv_count, 2, head_dim).astype(jnp.float32)
    own_keys = new_keys.reshape(count, kv_count, 2, head_dim).astype(jnp.float32)
    inv_scale = head_dim ** (-0.5)
    scores = jnp.einsum('bkgcd,bjkcd->bkgcj', query_grid, key_grid) * inv_scale
    own_score = jnp.einsum('bkgcd,bkcd->bkgc', query_grid, own_keys) * inv_scale
    visible = jnp.arange(ctx_len, dtype=jnp.int32)[None, :] < lengths[:, None]
    scores = jnp.where(visible[:, None, None, None, :], scores, masked_score)
    highest = jnp.maximum(lax.optimization_barrier(jnp.max(scores, axis=-1)), own_score)
    expd = jnp.exp(scores - highest[..., None])
    own_exp = jnp.exp(own_score - highest)
    denominator = lax.optimization_barrier(jnp.sum(expd, axis=-1)) + own_exp
    probs = expd / denominator[..., None]
    own_prob = own_exp / denominator
    lambda_grid = lambdas.reshape(kv_count, group)[None, :, :]
    weights = (probs[:, :, :, 0] - lambda_grid[..., None] * probs[:, :, :, 1]).astype(jnp.bfloat16)
    own_weight = (own_prob[..., 0] - lambda_grid * own_prob[..., 1]).astype(jnp.bfloat16)
    attended = jnp.einsum('bkgj,bjkv->bkgv', weights.astype(jnp.float32), cache_values.astype(jnp.float32))
    own_vals = new_values.reshape(count, kv_count, val_dim).astype(jnp.float32)
    attended = attended + own_weight.astype(jnp.float32)[..., None] * own_vals[:, :, None, :]
    return rms_scaled(attended, head_gain).reshape(count, heads * val_dim).astype(jnp.bfloat16)

def expert_mlp(inputs, gate_w, up_w, down_w):
    gate = jnp.dot(inputs, gate_w, preferred_element_type=jnp.float32)
    upper = jnp.dot(inputs, up_w, preferred_element_type=jnp.float32)
    gate = jnp.minimum(gate, clamp_limit)
    upper = jnp.clip(upper, -clamp_limit, clamp_limit)
    act = ((upper + 1.0) * gate * jax.nn.sigmoid(swish_alpha * gate)).astype(jnp.bfloat16)
    return jnp.dot(act, down_w, preferred_element_type=jnp.float32).astype(jnp.bfloat16)

def reference(tokens, norm_gain, query_weight, key_weight, value_weight, out_weight, head_gain, lambdas, cache_keys, cache_values, lengths, moe_gain, gate_weight, up_weight, down_weight, routes, route_weights):
    count = tokens.shape[0]
    width = tokens.shape[1]
    normed = rms_scaled(tokens, norm_gain).astype(jnp.bfloat16)
    queries = jnp.dot(normed, query_weight, preferred_element_type=jnp.float32).astype(jnp.bfloat16)
    new_keys = jnp.dot(normed, key_weight, preferred_element_type=jnp.float32).astype(jnp.bfloat16)
    new_values = jnp.dot(normed, value_weight, preferred_element_type=jnp.float32).astype(jnp.bfloat16)
    head_out = attention(queries, new_keys, new_values, cache_keys, cache_values, lengths, lambdas, head_gain)
    attn_out = jnp.dot(head_out, out_weight, preferred_element_type=jnp.float32).astype(jnp.bfloat16)
    residual = (tokens.astype(jnp.float32) + attn_out.astype(jnp.float32)).astype(jnp.bfloat16)
    moe_in = rms_scaled(residual, moe_gain).astype(jnp.bfloat16)
    onehot = (routes.reshape(N_EP, SEQ_DEV * TOPK)[:, :, None] == jnp.arange(EXPERTS, dtype=jnp.int32)[None, None, :]).astype(jnp.int32)
    earlier = jnp.cumsum(onehot, axis=1) - onehot
    ranks = lax.optimization_barrier(jnp.sum(earlier * onehot, axis=2)).reshape(count, TOPK)
    block_of = jnp.broadcast_to((jnp.arange(count, dtype=jnp.int32) // SEQ_DEV)[:, None], (count, TOPK))
    slot_index = (routes * (N_EP * CAP) + block_of * CAP + ranks).astype(jnp.int32).reshape(-1)
    copies = jnp.broadcast_to(moe_in[:, None, :], (count, TOPK, width)).reshape(-1, width)
    buffer = jnp.zeros((EXPERTS * N_EP * CAP, width), jnp.bfloat16).at[slot_index].set(copies)
    buffer = buffer.reshape(EXPERTS, N_EP * CAP, width)
    results = lax.map(lambda group: expert_mlp(group[0], group[1], group[2], group[3]), (buffer, gate_weight, up_weight, down_weight))
    picked = results.reshape(-1, width)[slot_index].reshape(count, TOPK, width)
    moe_sum = lax.optimization_barrier(jnp.sum(route_weights[:, :, None] * picked.astype(jnp.float32), axis=1))
    return (residual.astype(jnp.float32) + moe_sum).astype(jnp.bfloat16)
```

```python
import functools

import jax
import jax.numpy as jnp
from jax import lax
from jax.experimental import pallas as pl
from jax.experimental.pallas import tpu as pltpu
from jax.sharding import Mesh
from jax.sharding import PartitionSpec as P

EP = ("ep_0", "ep_1")
GRP_EP = ("grp", "ep_0", "ep_1")


epsilon = 1e-06
masked_score = -1e30
clamp_limit = 7.0
swish_alpha = 1.702


def rms_scaled(values, gain):
    floats = values.astype(jnp.float32)
    return (
        floats
        * lax.rsqrt(jnp.mean(floats * floats, axis=-1, keepdims=True) + epsilon)
        * gain.astype(jnp.float32)
    )


def core_swap(value):
    return lax.ppermute(value, "ep_1", [(0, 1), (1, 0)])


def ring_queries(normed, query_weight):
    count = normed.shape[0]
    chips = lax.axis_size("ep_0")
    cols = query_weight.shape[1]
    here = lax.axis_index("ep_0")
    core = lax.axis_index("ep_1")
    ahead = [(i, (i + 1) % chips) for i in range(chips)]
    behind = [(i, (i - 1) % chips) for i in range(chips)]
    both = jnp.concatenate([normed, core_swap(normed)], axis=0)

    def product(block):
        return jnp.dot(both, block, preferred_element_type=jnp.float32).astype(jnp.bfloat16)

    results = [None] * chips
    up = down = query_weight
    results[0] = product(query_weight)
    for step in range(1, chips // 2 + 1):
        up = lax.ppermute(up, "ep_0", ahead)
        if step < chips - step:
            down = lax.ppermute(down, "ep_0", behind)
        results[step] = product(up)
        if step < chips - step:
            results[chips - step] = product(down)
    stacked = jnp.stack(results[::-1])
    twice = jnp.concatenate([stacked, stacked], axis=0)
    placed = lax.dynamic_slice_in_dim(twice, chips - 1 - here, chips, axis=0)
    mine = placed[:, :count]
    theirs = core_swap(placed[:, count:])
    low = jnp.where(core == 0, mine, theirs)
    high = jnp.where(core == 0, theirs, mine)
    full = jnp.stack([low, high], axis=1)
    return jnp.transpose(full, (2, 0, 1, 3)).reshape(count, chips * 2 * cols)


def attention_kernel(
    group_size, chunk, lens_ref, q_ref, nk_ref, nv_ref, lam_ref, gain_ref, k_hbm, v_hbm, o_ref, k_buf, v_buf, k_sem, v_sem
):
    count, heads, width = q_ref.shape
    kv_count = nk_ref.shape[1]
    group = heads // kv_count
    half = width // 2
    rows = k_buf.shape[1]
    chunk_rows = chunk * kv_count
    chunks = rows // chunk_rows
    inv_scale = half ** (-0.5)

    def pieces(s, c):
        where = pl.ds(pl.multiple_of(c * chunk_rows, chunk_rows), chunk_rows)
        return (
            pltpu.make_async_copy(k_hbm.at[s, where], k_buf.at[s, where], k_sem.at[s]),
            pltpu.make_async_copy(v_hbm.at[s, where], v_buf.at[s, where], v_sem.at[s]),
        )

    def used(s):
        return (lens_ref[s] + chunk - 1) // chunk

    def fetch(s, _):
        n = used(s)

        def start(c, _):
            for copy in pieces(s, c):
                copy.start()
            return 0

        lax.fori_loop(0, n, start, 0)

        def clear(c, _):
            where = pl.ds(pl.multiple_of(c * chunk_rows, chunk_rows), chunk_rows)
            v_buf[s, where] = jnp.zeros((chunk_rows, width), v_buf.dtype)
            return 0

        lax.fori_loop(n, chunks, clear, 0)
        return 0

    lax.fori_loop(0, count, fetch, 0)

    lane = lax.broadcasted_iota(jnp.int32, (heads, width), 1)
    head_row = lax.broadcasted_iota(jnp.int32, (heads, width), 0)
    column = lax.broadcasted_iota(jnp.int32, (2 * heads, rows), 1)
    score_row = lax.broadcasted_iota(jnp.int32, (2 * heads, rows), 0)
    kv_of_row = (score_row % heads) // group
    own_kv = (column % kv_count) == kv_of_row
    position = column // kv_count
    gain = gain_ref[...].astype(jnp.float32)
    lam = lam_ref[...][:, :1]

    def spread(values):
        out = jnp.broadcast_to(values[kv_count - 1 :], (heads, width))
        for k in range(kv_count - 1):
            out = jnp.where(head_row // group == k, jnp.broadcast_to(values[k : k + 1], (heads, width)), out)
        return out

    def one(s):
        q = q_ref[s]
        zero = jnp.zeros_like(q)
        split = jnp.concatenate([jnp.where(lane < half, q, zero), jnp.where(lane < half, zero, q)], axis=0)
        own_key = spread(nk_ref[s].astype(jnp.float32))
        own_val = spread(nv_ref[s].astype(jnp.float32))
        own_score = (
            jnp.sum(split.astype(jnp.float32) * jnp.concatenate([own_key, own_key], axis=0), axis=1, keepdims=True)
            * inv_scale
        )
        scores = (
            lax.dot_general(split, k_buf[s], (((1,), (1,)), ((), ())), preferred_element_type=jnp.float32) * inv_scale
        )
        scores = jnp.where(own_kv & (position < lens_ref[s]), scores, masked_score)
        highest = jnp.maximum(jnp.max(scores, axis=1, keepdims=True), own_score)
        expd = jnp.exp(scores - highest)
        own_exp = jnp.exp(own_score - highest)
        denominator = jnp.sum(expd, axis=1, keepdims=True) + own_exp
        inverse = 1.0 / denominator
        factor = inverse[heads:] * lam
        weights = (expd[:heads] * inverse[:heads] - expd[heads:] * factor).astype(jnp.bfloat16)
        own_weight = (own_exp[:heads] * inverse[:heads] - own_exp[heads:] * factor).astype(jnp.bfloat16)
        attended = jnp.dot(weights, v_buf[s], preferred_element_type=jnp.float32)
        attended = attended + own_weight.astype(jnp.float32) * own_val
        scale = lax.rsqrt(jnp.mean(attended * attended, axis=1, keepdims=True) + epsilon)
        o_ref[s] = (attended * scale * gain).astype(o_ref.dtype)

    def step(g, _):
        for i in range(group_size):
            s = g * group_size + i

            def wait(c, _):
                for copy in pieces(s, c):
                    copy.wait()
                return 0

            lax.fori_loop(0, used(s), wait, 0)
        for i in range(group_size):
            one(g * group_size + i)
        return 0

    lax.fori_loop(0, count // group_size, step, 0)


def attention(queries, new_keys, new_values, cache_keys, cache_values, lengths, lambdas, head_gain):
    count, ctx_len, kv_count, width = cache_keys.shape
    heads = lambdas.shape[0]
    vmem = pl.BlockSpec(memory_space=pltpu.VMEM)
    smem = pl.BlockSpec(memory_space=pltpu.SMEM)
    hbm = pl.BlockSpec(memory_space=pl.ANY)
    rows = ctx_len * kv_count
    out = pl.pallas_call(
        functools.partial(attention_kernel, 2, 128),
        out_shape=jax.ShapeDtypeStruct((count, heads, width), jnp.bfloat16),
        in_specs=[smem, vmem, vmem, vmem, vmem, vmem, hbm, hbm],
        out_specs=vmem,
        scratch_shapes=[
            pltpu.VMEM((count, rows, width), jnp.bfloat16),
            pltpu.VMEM((count, rows, width), jnp.bfloat16),
            pltpu.SemaphoreType.DMA((count,)),
            pltpu.SemaphoreType.DMA((count,)),
        ],
        compiler_params=pltpu.CompilerParams(vmem_limit_bytes=40 * 2**20),
        name="attention",
    )(
        lengths,
        queries.reshape(count, heads, width),
        new_keys.reshape(count, kv_count, width),
        new_values.reshape(count, kv_count, width),
        jnp.broadcast_to(lambdas[:, None], (heads, width)),
        head_gain.reshape(1, width),
        cache_keys.reshape(count, rows, width),
        cache_values.reshape(count, rows, width),
    )
    return out.reshape(count, heads * width)


def expert_mlp(inputs, gate_w, up_w, down_w):
    gate = jnp.dot(inputs, gate_w, preferred_element_type=jnp.float32)
    upper = jnp.dot(inputs, up_w, preferred_element_type=jnp.float32)
    gate = jnp.minimum(gate, clamp_limit)
    upper = jnp.clip(upper, -clamp_limit, clamp_limit)
    act = ((upper + 1.0) * gate * jax.nn.sigmoid(swish_alpha * gate)).astype(jnp.bfloat16)
    return jnp.dot(act, down_w, preferred_element_type=jnp.float32).astype(jnp.bfloat16)


def local(
    tokens,
    norm_gain,
    query_weight,
    key_weight,
    value_weight,
    out_weight,
    head_gain,
    lambdas,
    cache_keys,
    cache_values,
    lengths,
    moe_gain,
    gate_weight,
    up_weight,
    down_weight,
    routes,
    route_weights,
):
    count = tokens.shape[0]
    width = tokens.shape[1]
    topk = routes.shape[1]
    out_full = lax.all_gather(out_weight, EP, axis=1, tiled=True)
    normed = rms_scaled(tokens, norm_gain).astype(jnp.bfloat16)
    new_keys = jnp.dot(normed, key_weight, preferred_element_type=jnp.float32).astype(jnp.bfloat16)
    new_values = jnp.dot(normed, value_weight, preferred_element_type=jnp.float32).astype(
        jnp.bfloat16
    )
    queries = ring_queries(normed, query_weight)
    head_out = attention(
        queries, new_keys, new_values, cache_keys, cache_values, lengths, lambdas, head_gain
    )
    attn_out = jnp.dot(head_out, out_full, preferred_element_type=jnp.float32).astype(jnp.bfloat16)
    residual = (tokens.astype(jnp.float32) + attn_out.astype(jnp.float32)).astype(jnp.bfloat16)
    moe_in = rms_scaled(residual, moe_gain).astype(jnp.bfloat16)
    experts = lax.axis_size(EP)
    capacity = min(count, max(2, 2 * count * topk // experts))
    onehot = (routes.reshape(-1)[:, None] == jnp.arange(experts, dtype=jnp.int32)[None, :]).astype(
        jnp.int32
    )
    earlier_all = jnp.cumsum(onehot, axis=0) - onehot
    ranks = jnp.sum(earlier_all * onehot, axis=1).reshape(count, topk)
    slot_id = routes * capacity + ranks
    slot_range = jnp.arange(experts * capacity, dtype=jnp.int32)
    dispatch = jnp.any(slot_id[None, :, :] == slot_range[:, None, None], axis=2).astype(
        jnp.bfloat16
    )
    outgoing = jnp.dot(dispatch, moe_in, preferred_element_type=jnp.float32).astype(jnp.bfloat16)
    outgoing = outgoing.reshape(experts, capacity, width)
    received = lax.all_to_all(outgoing, EP, split_axis=0, concat_axis=0, tiled=True)
    flat_rows = received.reshape(-1, width)
    results = expert_mlp(flat_rows, gate_weight[0], up_weight[0], down_weight[0]).reshape(
        received.shape
    )
    returned = lax.all_to_all(results, EP, split_axis=0, concat_axis=0, tiled=True)
    picked = returned.reshape(-1, width)[slot_id].astype(jnp.float32)
    moe_sum = jnp.sum(route_weights[:, :, None] * picked, axis=1)
    return (residual.astype(jnp.float32) + moe_sum).astype(jnp.bfloat16)


def solution(mesh):
    chips = mesh.shape["ep"] // 2
    torus = Mesh(mesh.devices.reshape(mesh.shape["grp"], chips, 2), ("grp", "ep_0", "ep_1"))
    return jax.shard_map(
        local,
        mesh=torus,
        in_specs=(
            P(GRP_EP, None),
            P(),
            P(None, EP),
            P(),
            P(),
            P(None, EP),
            P(),
            P(),
            P(GRP_EP, None, None, None),
            P(GRP_EP, None, None, None),
            P(GRP_EP),
            P(),
            P(EP, None, None),
            P(EP, None, None),
            P(EP, None, None),
            P(GRP_EP, None),
            P(GRP_EP, None),
        ),
        out_specs=P(GRP_EP, None),
        check_vma=False,
    )
```

```python
import functools

import jax
import jax.numpy as jnp
from jax import lax
from jax.experimental import pallas as pl
from jax.experimental.pallas import tpu as pltpu
from jax.sharding import Mesh
from jax.sharding import PartitionSpec as P

EP = ("far", "near", "core")
NEAR = ("near", "core")
GRP_EP = ("grp", "far", "near", "core")


epsilon = 1e-06
masked_score = -1e30
clamp_limit = 7.0
swish_alpha = 1.702


def rms_scaled(values, gain):
    floats = values.astype(jnp.float32)
    return (
        floats
        * lax.rsqrt(jnp.mean(floats * floats, axis=-1, keepdims=True) + epsilon)
        * gain.astype(jnp.float32)
    )


def far_blocks(block):
    size = lax.axis_size("far")
    out = [block]
    for d in range(1, size):
        out.append(lax.ppermute(block, "far", [(i, (i + d) % size) for i in range(size)]))
    return out


def near_product(rows, blocks):
    members = lax.axis_size(NEAR)
    size = len(blocks)
    here = lax.axis_index("far")
    cols = blocks[0].shape[1]
    count = rows.shape[0] // members
    parts = [
        jnp.dot(rows, block, preferred_element_type=jnp.float32).astype(jnp.bfloat16)
        for block in blocks
    ]
    stacked = jnp.stack(parts[::-1] + parts[::-1])
    placed = lax.dynamic_slice_in_dim(stacked, size - 1 - here, size, axis=0)
    outgoing = jnp.transpose(placed.reshape(size, members, count, cols), (1, 2, 0, 3))
    received = lax.all_to_all(
        outgoing.reshape(members, count, size * cols), NEAR, 0, 0, tiled=True
    ).reshape(members, count, size, cols)
    return jnp.transpose(received, (1, 2, 0, 3)).reshape(count, size * members * cols)


def attention_kernel(
    group_size, chunk, lens_ref, q_ref, nk_ref, nv_ref, lam_ref, gain_ref, k_hbm, v_hbm, o_ref, k_buf, v_buf, k_sem, v_sem
):
    count, heads, width = q_ref.shape
    kv_count = nk_ref.shape[1]
    group = heads // kv_count
    half = width // 2
    rows = k_buf.shape[1]
    chunk_rows = chunk * kv_count
    chunks = rows // chunk_rows
    inv_scale = half ** (-0.5)

    def pieces(s, c):
        where = pl.ds(pl.multiple_of(c * chunk_rows, chunk_rows), chunk_rows)
        return (
            pltpu.make_async_copy(k_hbm.at[s, where], k_buf.at[s, where], k_sem.at[s]),
            pltpu.make_async_copy(v_hbm.at[s, where], v_buf.at[s, where], v_sem.at[s]),
        )

    def used(s):
        return (lens_ref[s] + chunk - 1) // chunk

    def fetch(s, _):
        n = used(s)

        def start(c, _):
            for copy in pieces(s, c):
                copy.start()
            return 0

        lax.fori_loop(0, n, start, 0)

        def clear(c, _):
            where = pl.ds(pl.multiple_of(c * chunk_rows, chunk_rows), chunk_rows)
            v_buf[s, where] = jnp.zeros((chunk_rows, width), v_buf.dtype)
            return 0

        lax.fori_loop(n, chunks, clear, 0)
        return 0

    lax.fori_loop(0, count, fetch, 0)

    lane = lax.broadcasted_iota(jnp.int32, (heads, width), 1)
    head_row = lax.broadcasted_iota(jnp.int32, (heads, width), 0)
    column = lax.broadcasted_iota(jnp.int32, (2 * heads, rows), 1)
    score_row = lax.broadcasted_iota(jnp.int32, (2 * heads, rows), 0)
    kv_of_row = (score_row % heads) // group
    own_kv = (column % kv_count) == kv_of_row
    position = column // kv_count
    gain = gain_ref[...].astype(jnp.float32)
    lam = lam_ref[...][:, :1]

    def spread(values):
        out = jnp.broadcast_to(values[kv_count - 1 :], (heads, width))
        for k in range(kv_count - 1):
            out = jnp.where(head_row // group == k, jnp.broadcast_to(values[k : k + 1], (heads, width)), out)
        return out

    def one(s):
        q = q_ref[s]
        zero = jnp.zeros_like(q)
        split = jnp.concatenate([jnp.where(lane < half, q, zero), jnp.where(lane < half, zero, q)], axis=0)
        own_key = spread(nk_ref[s].astype(jnp.float32))
        own_val = spread(nv_ref[s].astype(jnp.float32))
        own_score = (
            jnp.sum(split.astype(jnp.float32) * jnp.concatenate([own_key, own_key], axis=0), axis=1, keepdims=True)
            * inv_scale
        )
        scores = (
            lax.dot_general(split, k_buf[s], (((1,), (1,)), ((), ())), preferred_element_type=jnp.float32) * inv_scale
        )
        scores = jnp.where(own_kv & (position < lens_ref[s]), scores, masked_score)
        highest = jnp.maximum(jnp.max(scores, axis=1, keepdims=True), own_score)
        expd = jnp.exp(scores - highest)
        own_exp = jnp.exp(own_score - highest)
        denominator = jnp.sum(expd, axis=1, keepdims=True) + own_exp
        inverse = 1.0 / denominator
        factor = inverse[heads:] * lam
        weights = (expd[:heads] * inverse[:heads] - expd[heads:] * factor).astype(jnp.bfloat16)
        own_weight = (own_exp[:heads] * inverse[:heads] - own_exp[heads:] * factor).astype(jnp.bfloat16)
        attended = jnp.dot(weights, v_buf[s], preferred_element_type=jnp.float32)
        attended = attended + own_weight.astype(jnp.float32) * own_val
        scale = lax.rsqrt(jnp.mean(attended * attended, axis=1, keepdims=True) + epsilon)
        o_ref[s] = (attended * scale * gain).astype(o_ref.dtype)

    def step(g, _):
        for i in range(group_size):
            s = g * group_size + i

            def wait(c, _):
                for copy in pieces(s, c):
                    copy.wait()
                return 0

            lax.fori_loop(0, used(s), wait, 0)
        for i in range(group_size):
            one(g * group_size + i)
        return 0

    lax.fori_loop(0, count // group_size, step, 0)


def attention(queries, new_keys, new_values, cache_keys, cache_values, lengths, lambdas, head_gain):
    count, ctx_len, kv_count, width = cache_keys.shape
    heads = lambdas.shape[0]
    vmem = pl.BlockSpec(memory_space=pltpu.VMEM)
    smem = pl.BlockSpec(memory_space=pltpu.SMEM)
    hbm = pl.BlockSpec(memory_space=pltpu.HBM)
    rows = ctx_len * kv_count
    out = pl.pallas_call(
        functools.partial(attention_kernel, 2, 128),
        out_shape=jax.ShapeDtypeStruct((count, heads, width), jnp.bfloat16),
        in_specs=[smem, vmem, vmem, vmem, vmem, vmem, hbm, hbm],
        out_specs=vmem,
        scratch_shapes=[
            pltpu.VMEM((count, rows, width), jnp.bfloat16),
            pltpu.VMEM((count, rows, width), jnp.bfloat16),
            pltpu.SemaphoreType.DMA((count,)),
            pltpu.SemaphoreType.DMA((count,)),
        ],
        compiler_params=pltpu.CompilerParams(vmem_limit_bytes=40 * 2**20),
        name="attention",
    )(
        lengths,
        queries.reshape(count, heads, width),
        new_keys.reshape(count, kv_count, width),
        new_values.reshape(count, kv_count, width),
        jnp.broadcast_to(lambdas[:, None], (heads, width)),
        head_gain.reshape(1, width),
        cache_keys.reshape(count, rows, width),
        cache_values.reshape(count, rows, width),
    )
    return out.reshape(count, heads * width)


def expert_mlp(inputs, gate_w, up_w, down_w):
    gate = jnp.dot(inputs, gate_w, preferred_element_type=jnp.float32)
    upper = jnp.dot(inputs, up_w, preferred_element_type=jnp.float32)
    gate = jnp.minimum(gate, clamp_limit)
    upper = jnp.clip(upper, -clamp_limit, clamp_limit)
    act = ((upper + 1.0) * gate * jax.nn.sigmoid(swish_alpha * gate)).astype(jnp.bfloat16)
    return jnp.dot(act, down_w, preferred_element_type=jnp.float32).astype(jnp.bfloat16)


def local(
    tokens,
    norm_gain,
    query_weight,
    key_weight,
    value_weight,
    out_weight,
    head_gain,
    lambdas,
    cache_keys,
    cache_values,
    lengths,
    moe_gain,
    gate_weight,
    up_weight,
    down_weight,
    routes,
    route_weights,
):
    count = tokens.shape[0]
    width = tokens.shape[1]
    topk = routes.shape[1]
    query_blocks = far_blocks(query_weight)
    normed = rms_scaled(tokens, norm_gain).astype(jnp.bfloat16)
    new_keys = jnp.dot(normed, key_weight, preferred_element_type=jnp.float32).astype(jnp.bfloat16)
    new_values = jnp.dot(normed, value_weight, preferred_element_type=jnp.float32).astype(
        jnp.bfloat16
    )
    near_normed = lax.all_gather(normed, NEAR, axis=0, tiled=True)
    held, *query_blocks = lax.optimization_barrier((out_weight, *query_blocks))
    out_blocks = far_blocks(held)
    queries = near_product(near_normed, query_blocks)
    head_out = attention(
        queries, new_keys, new_values, cache_keys, cache_values, lengths, lambdas, head_gain
    )
    near_heads = lax.all_gather(head_out, NEAR, axis=0, tiled=True)
    attn_out = near_product(near_heads, out_blocks)
    residual = (tokens.astype(jnp.float32) + attn_out.astype(jnp.float32)).astype(jnp.bfloat16)
    moe_in = rms_scaled(residual, moe_gain).astype(jnp.bfloat16)
    experts = lax.axis_size(EP)
    capacity = min(count, max(2, 2 * count * topk // experts))
    onehot = (routes.reshape(-1)[:, None] == jnp.arange(experts, dtype=jnp.int32)[None, :]).astype(
        jnp.int32
    )
    earlier_all = jnp.cumsum(onehot, axis=0) - onehot
    ranks = jnp.sum(earlier_all * onehot, axis=1).reshape(count, topk)
    slot_id = routes * capacity + ranks
    slot_range = jnp.arange(experts * capacity, dtype=jnp.int32)
    dispatch = jnp.any(slot_id[None, :, :] == slot_range[:, None, None], axis=2).astype(
        jnp.bfloat16
    )
    outgoing = jnp.dot(dispatch, moe_in, preferred_element_type=jnp.float32).astype(jnp.bfloat16)
    outgoing = outgoing.reshape(experts, capacity, width)
    received = lax.all_to_all(outgoing, EP, split_axis=0, concat_axis=0, tiled=True)
    flat_rows = received.reshape(-1, width)
    results = expert_mlp(flat_rows, gate_weight[0], up_weight[0], down_weight[0]).reshape(
        received.shape
    )
    returned = lax.all_to_all(results, EP, split_axis=0, concat_axis=0, tiled=True)
    picked = returned.reshape(-1, width)[slot_id].astype(jnp.float32)
    moe_sum = jnp.sum(route_weights[:, :, None] * picked, axis=1)
    return (residual.astype(jnp.float32) + moe_sum).astype(jnp.bfloat16)


def solution(mesh):
    devices = mesh.devices.reshape(mesh.shape["grp"], -1, 4, 2)
    torus = Mesh(devices, ("grp", "far", "near", "core"))
    return jax.shard_map(
        local,
        mesh=torus,
        in_specs=(
            P(GRP_EP, None),
            P(),
            P(None, EP),
            P(),
            P(),
            P(None, EP),
            P(),
            P(),
            P(GRP_EP, None, None, None),
            P(GRP_EP, None, None, None),
            P(GRP_EP),
            P(),
            P(EP, None, None),
            P(EP, None, None),
            P(EP, None, None),
            P(GRP_EP, None),
            P(GRP_EP, None),
        ),
        out_specs=P(GRP_EP, None),
        check_vma=False,
    )
```

```python
import functools

import jax
import jax.numpy as jnp
from jax import lax
from jax.experimental import pallas as pl
from jax.experimental.pallas import tpu as pltpu
from jax.sharding import Mesh
from jax.sharding import PartitionSpec as P

EP = ("far", "near", "core")
NEAR = ("near", "core")
CHIPS = ("far", "near")
GRP_EP = ("grp", "far", "near", "core")


epsilon = 1e-06
masked_score = -1e30
clamp_limit = 7.0
swish_alpha = 1.702


def rms_scaled(values, gain):
    floats = values.astype(jnp.float32)
    return (
        floats
        * lax.rsqrt(jnp.mean(floats * floats, axis=-1, keepdims=True) + epsilon)
        * gain.astype(jnp.float32)
    )


def far_blocks(block):
    size = lax.axis_size("far")
    out = [block]
    for d in range(1, size):
        out.append(lax.ppermute(block, "far", [(i, (i + d) % size) for i in range(size)]))
    return out


def near_product(rows, blocks):
    members = lax.axis_size(NEAR)
    size = len(blocks)
    here = lax.axis_index("far")
    cols = blocks[0].shape[1]
    count = rows.shape[0] // members
    parts = [
        jnp.dot(rows, block, preferred_element_type=jnp.float32).astype(jnp.bfloat16)
        for block in blocks
    ]
    stacked = jnp.stack(parts[::-1] + parts[::-1])
    placed = lax.dynamic_slice_in_dim(stacked, size - 1 - here, size, axis=0)
    outgoing = jnp.transpose(placed.reshape(size, members, count, cols), (1, 2, 0, 3))
    received = lax.all_to_all(
        outgoing.reshape(members, count, size * cols), NEAR, 0, 0, tiled=True
    ).reshape(members, count, size, cols)
    return jnp.transpose(received, (1, 2, 0, 3)).reshape(count, size * members * cols)


def attention_kernel(
    group_size, chunk, lens_ref, q_ref, nk_ref, nv_ref, lam_ref, gain_ref, k_hbm, v_hbm, o_ref, k_buf, v_buf, s_buf, k_sem, v_sem
):
    count, heads, width = q_ref.shape
    kv_count = nk_ref.shape[1]
    group = heads // kv_count
    half = width // 2
    rows = k_buf.shape[1]
    chunk_rows = chunk * kv_count
    chunks = rows // chunk_rows
    inv_scale = half ** (-0.5)

    def piece(s, c):
        return pl.ds(pl.multiple_of(c * chunk_rows, chunk_rows), chunk_rows)

    def copies(s, where):
        return (
            pltpu.make_async_copy(k_hbm.at[s, where], k_buf.at[s, where], k_sem.at[s]),
            pltpu.make_async_copy(v_hbm.at[s, where], v_buf.at[s, where], v_sem.at[s]),
        )

    def used(s):
        return (lens_ref[s] + chunk - 1) // chunk

    def fetch(s, _):
        n = used(s)
        for c in range(chunks):
            where = pl.ds(c * chunk_rows, chunk_rows)

            @pl.when(c < n)
            def _():
                for copy in copies(s, where):
                    copy.start()

            @pl.when(c >= n)
            def _():
                v_buf[s, where] = jnp.zeros((chunk_rows, width), v_buf.dtype)

        return 0

    lax.fori_loop(0, count, fetch, 0)

    lane = lax.broadcasted_iota(jnp.int32, (heads, width), 1)
    head_row = lax.broadcasted_iota(jnp.int32, (heads, width), 0)
    column = lax.broadcasted_iota(jnp.int32, (1, heads, rows), 2)
    score_head = lax.broadcasted_iota(jnp.int32, (1, heads, rows), 1)
    own_kv = (column % kv_count) == score_head // group
    position = jnp.where(own_kv, column // kv_count, rows)[None]
    gain = gain_ref[...].astype(jnp.float32)
    lam = lam_ref[...][None, :, :1]
    low = (lane < half)[None]
    block = lax.broadcasted_iota(jnp.int32, (group_size, 1, heads, 1), 0)

    def spread(values):
        out = jnp.broadcast_to(values[:, kv_count - 1 :], (group_size, heads, width))
        for k in range(kv_count - 1):
            out = jnp.where((head_row // group == k)[None], values[:, k : k + 1], out)
        return out

    def step(g, _):
        first = g * group_size
        here = pl.ds(first, group_size)
        q = q_ref[here]
        zero = jnp.zeros_like(q)
        split = jnp.stack([jnp.where(low, q, zero), jnp.where(low, zero, q)], axis=1)
        own_key = spread(nk_ref[here].astype(jnp.float32))
        own_val = spread(nv_ref[here].astype(jnp.float32))
        own_score = (
            jnp.sum(split.astype(jnp.float32) * own_key[:, None], axis=3, keepdims=True) * inv_scale
        )
        limit = jnp.zeros((group_size, 1, heads, 1), jnp.int32)
        for i in range(group_size):
            s = first + i
            limit = jnp.where(block == i, lens_ref[s], limit)

            def wait(c, _):
                for copy in copies(s, piece(s, c)):
                    copy.wait()
                return 0

            lax.fori_loop(0, used(s), wait, 0)
        for i in range(group_size):
            s_buf[i] = lax.dot_general(
                split[i].reshape(2 * heads, width), k_buf[first + i], (((1,), (1,)), ((), ())), preferred_element_type=jnp.float32
            ).reshape(2, heads, rows)
        scores = jnp.where(position < limit, s_buf[...] * inv_scale, masked_score)
        highest = jnp.maximum(jnp.max(scores, axis=3, keepdims=True), own_score)
        expd = jnp.exp(scores - highest)
        own_exp = jnp.exp(own_score - highest)
        inverse = 1.0 / (jnp.sum(expd, axis=3, keepdims=True) + own_exp)
        plus = inverse[:, 0]
        minus = inverse[:, 1] * lam
        weights = (expd[:, 0] * plus - expd[:, 1] * minus).astype(jnp.bfloat16)
        own_weight = (own_exp[:, 0] * plus - own_exp[:, 1] * minus).astype(jnp.bfloat16)
        attended = jnp.stack(
            [
                jnp.dot(weights[i], v_buf[first + i], preferred_element_type=jnp.float32)
                for i in range(group_size)
            ]
        )
        attended = attended + own_weight.astype(jnp.float32) * own_val
        scale = lax.rsqrt(jnp.mean(attended * attended, axis=2, keepdims=True) + epsilon)
        o_ref[here] = (attended * scale * gain[None]).astype(o_ref.dtype)
        return 0

    lax.fori_loop(0, count // group_size, step, 0)


def attention(queries, new_keys, new_values, cache_keys, cache_values, lengths, lambdas, head_gain):
    count, ctx_len, kv_count, width = cache_keys.shape
    heads = lambdas.shape[0]
    vmem = pl.BlockSpec(memory_space=pltpu.VMEM)
    smem = pl.BlockSpec(memory_space=pltpu.SMEM)
    hbm = pl.BlockSpec(memory_space=pltpu.HBM)
    rows = ctx_len * kv_count
    together = 8
    out = pl.pallas_call(
        functools.partial(attention_kernel, together, 128),
        out_shape=jax.ShapeDtypeStruct((count, heads, width), jnp.bfloat16),
        in_specs=[smem, vmem, vmem, vmem, vmem, vmem, hbm, hbm],
        out_specs=vmem,
        scratch_shapes=[
            pltpu.VMEM((count, rows, width), jnp.bfloat16),
            pltpu.VMEM((count, rows, width), jnp.bfloat16),
            pltpu.VMEM((together, 2, heads, rows), jnp.float32),
            pltpu.SemaphoreType.DMA((count,)),
            pltpu.SemaphoreType.DMA((count,)),
        ],
        compiler_params=pltpu.CompilerParams(vmem_limit_bytes=60 * 2**20),
        name="attention",
    )(
        lengths,
        queries.reshape(count, heads, width),
        new_keys.reshape(count, kv_count, width),
        new_values.reshape(count, kv_count, width),
        jnp.broadcast_to(lambdas[:, None], (heads, width)),
        head_gain.reshape(1, width),
        cache_keys.reshape(count, rows, width),
        cache_values.reshape(count, rows, width),
    )
    return out.reshape(count, heads * width)


def expert_kernel(
    core_ref, h_ref, own_ref, tok_ref, gain_ref, near_hbm, other_hbm, gate_hbm, up_hbm, down_hbm,
    o_ref, res_ref, wo_buf, x_buf, gate_buf, up_buf, down_buf, wo_sem, x_sem, gate_sem, up_sem, down_sem,
):
    core = core_ref[0]
    cols = wo_buf.shape[1] // 2
    depth = wo_buf.shape[2]
    count = own_ref.shape[0]
    slots = h_ref.shape[0]
    members = x_buf.shape[1] * 2
    halves = x_buf.shape[0]
    pieces = down_sem.shape[0]
    width = o_ref.shape[1]
    step = width // pieces

    wo_copies = []
    x_copies = []
    for i, source in enumerate((near_hbm, other_hbm)):
        side = core if i == 0 else 1 - core
        at = pl.ds(pl.multiple_of(side * cols, cols), cols)
        wo_copies.append(
            pltpu.make_async_copy(source.at[:, pl.ds(0, cols)], wo_buf.at[:, at], wo_sem.at[i])
        )
        at = pl.ds(pl.multiple_of(side * count, count), count)
        for half in range(halves):
            rows = pl.ds(cols + half * count, count)
            x_copies.append(
                pltpu.make_async_copy(
                    source.at[:, rows], x_buf.at[half, :, at], x_sem.at[i * halves + half]
                )
            )
    gate_copy = pltpu.make_async_copy(gate_hbm.at[0], gate_buf, gate_sem)
    up_copy = pltpu.make_async_copy(up_hbm.at[0], up_buf, up_sem)
    down_copies = [
        pltpu.make_async_copy(
            down_hbm.at[0, :, pl.ds(i * step, step)], down_buf.at[:, pl.ds(i * step, step)], down_sem.at[i]
        )
        for i in range(pieces)
    ]
    for copy in (*wo_copies, *x_copies, gate_copy, up_copy, *down_copies):
        copy.start()

    heads = jnp.concatenate([h_ref[:, :depth], own_ref[...]], axis=0)
    chosen = h_ref[:, depth:]
    lanes = chosen.shape[1]
    per = slots // members
    token = lax.broadcasted_iota(jnp.int32, (lanes, members * count), 0)
    column = lax.broadcasted_iota(jnp.int32, (lanes, members * count), 1)
    repeat = jnp.where(column % count == token, 1.0, 0.0).astype(jnp.bfloat16)
    spread = jnp.dot(chosen, repeat, preferred_element_type=jnp.float32)
    slot = lax.broadcasted_iota(jnp.int32, (slots, members * count), 0)
    column = lax.broadcasted_iota(jnp.int32, (slots, members * count), 1)
    select = jnp.where(slot // per == column // count, spread, 0.0).astype(jnp.bfloat16)

    for copy in wo_copies:
        copy.wait()
    attn = lax.dot_general(
        heads,
        wo_buf[...].reshape(width, depth),
        (((1,), (1,)), ((), ())),
        preferred_element_type=jnp.float32,
    ).astype(jnp.bfloat16)
    res_ref[...] = (
        tok_ref[...].astype(jnp.float32) + attn[slots:].astype(jnp.float32)
    ).astype(res_ref.dtype)
    for copy in x_copies:
        copy.wait()
    rows = jnp.concatenate(
        [
            jnp.dot(
                select,
                x_buf[half].reshape(members * count, depth),
                preferred_element_type=jnp.float32,
            )
            for half in range(halves)
        ],
        axis=1,
    )
    residual = (rows + attn[:slots].astype(jnp.float32)).astype(jnp.bfloat16)
    inputs = rms_scaled(residual, gain_ref[...]).astype(jnp.bfloat16)
    gate_copy.wait()
    gate = jnp.dot(inputs, gate_buf[...], preferred_element_type=jnp.float32)
    gate = jnp.minimum(gate, clamp_limit)
    swish = gate * (1.0 / (1.0 + jnp.exp(-swish_alpha * gate)))
    up_copy.wait()
    upper = jnp.dot(inputs, up_buf[...], preferred_element_type=jnp.float32)
    upper = jnp.clip(upper, -clamp_limit, clamp_limit)
    act = ((upper + 1.0) * swish).astype(jnp.bfloat16)
    for i, copy in enumerate(down_copies):
        copy.wait()
        at = pl.ds(i * step, step)
        o_ref[:, at] = jnp.dot(act, down_buf[:, at], preferred_element_type=jnp.float32).astype(
            o_ref.dtype
        )


def expert(core, received, head_out, tokens, moe_gain, near, other, gate_w, up_w, down_w):
    slots = received.shape[0]
    count, width = tokens.shape
    chips, packed, depth = near.shape
    halves = width // depth
    cols = packed - halves * count
    hidden = gate_w.shape[2]
    pieces = 4
    vmem = pl.BlockSpec(memory_space=pltpu.VMEM)
    smem = pl.BlockSpec(memory_space=pltpu.SMEM)
    hbm = pl.BlockSpec(memory_space=pltpu.HBM)
    bf16 = jnp.bfloat16
    return pl.pallas_call(
        expert_kernel,
        out_shape=(
            jax.ShapeDtypeStruct((slots, width), bf16),
            jax.ShapeDtypeStruct((count, width), bf16),
        ),
        in_specs=[smem, vmem, vmem, vmem, vmem, hbm, hbm, hbm, hbm, hbm],
        out_specs=(vmem, vmem),
        scratch_shapes=[
            pltpu.VMEM((chips, 2 * cols, depth), bf16),
            pltpu.VMEM((halves, chips, 2 * count, depth), bf16),
            pltpu.VMEM((width, hidden), bf16),
            pltpu.VMEM((width, hidden), bf16),
            pltpu.VMEM((hidden, width), bf16),
            pltpu.SemaphoreType.DMA((2,)),
            pltpu.SemaphoreType.DMA((2 * halves,)),
            pltpu.SemaphoreType.DMA,
            pltpu.SemaphoreType.DMA,
            pltpu.SemaphoreType.DMA((pieces,)),
        ],
        compiler_params=pltpu.CompilerParams(vmem_limit_bytes=60 * 2**20),
        name="expert",
    )(core, received, head_out, tokens, moe_gain.reshape(1, width), near, other, gate_w, up_w, down_w)


def combine_kernel(share_ref, rows_ref, res_ref, o_ref):
    share = share_ref[...]
    high = share.astype(jnp.bfloat16)
    low = (share - high.astype(jnp.float32)).astype(jnp.bfloat16)
    rows = rows_ref[...]
    total = jnp.dot(high, rows, preferred_element_type=jnp.float32) + jnp.dot(
        low, rows, preferred_element_type=jnp.float32
    )
    o_ref[...] = (res_ref[...].astype(jnp.float32) + total).astype(o_ref.dtype)


def combine(share, rows, residual):
    vmem = pl.BlockSpec(memory_space=pltpu.VMEM)
    return pl.pallas_call(
        combine_kernel,
        out_shape=jax.ShapeDtypeStruct(residual.shape, jnp.bfloat16),
        in_specs=[vmem] * 3,
        out_specs=vmem,
        name="combine",
    )(share, rows, residual)


def local(
    tokens,
    norm_gain,
    query_weight,
    key_weight,
    value_weight,
    out_weight,
    head_gain,
    lambdas,
    cache_keys,
    cache_values,
    lengths,
    moe_gain,
    gate_weight,
    up_weight,
    down_weight,
    routes,
    route_weights,
):
    count = tokens.shape[0]
    topk = routes.shape[1]
    depth = out_weight.shape[0]
    packed = jnp.concatenate([out_weight.T, tokens[:, :depth], tokens[:, depth:]], axis=0)
    near_packed = lax.all_gather(packed, CHIPS, axis=0)
    query_blocks = far_blocks(query_weight)
    normed = rms_scaled(tokens, norm_gain).astype(jnp.bfloat16)
    new_keys = jnp.dot(normed, key_weight, preferred_element_type=jnp.float32).astype(jnp.bfloat16)
    new_values = jnp.dot(normed, value_weight, preferred_element_type=jnp.float32).astype(
        jnp.bfloat16
    )
    near_normed = lax.all_gather(normed, NEAR, axis=0, tiled=True)
    queries = near_product(near_normed, query_blocks)
    head_out = attention(
        queries, new_keys, new_values, cache_keys, cache_values, lengths, lambdas, head_gain
    )
    experts = lax.axis_size(EP)
    capacity = min(count, max(2, 2 * count * topk // experts))
    onehot = (routes.reshape(-1)[:, None] == jnp.arange(experts, dtype=jnp.int32)[None, :]).astype(
        jnp.int32
    )
    earlier_all = jnp.cumsum(onehot, axis=0) - onehot
    ranks = jnp.sum(earlier_all * onehot, axis=1).reshape(count, topk)
    slot_id = routes * capacity + ranks
    slot_range = jnp.arange(experts * capacity, dtype=jnp.int32)
    dispatch = jnp.any(slot_id[None, :, :] == slot_range[:, None, None], axis=2).astype(
        jnp.bfloat16
    )
    share = jnp.sum(
        jnp.where(slot_id[:, :, None] == slot_range[None, None, :], route_weights[:, :, None], 0.0),
        axis=1,
    )
    outgoing = jnp.concatenate(
        [
            jnp.dot(dispatch, head_out, preferred_element_type=jnp.float32).astype(jnp.bfloat16),
            jnp.pad(dispatch, ((0, 0), (0, 128 - count))),
        ],
        axis=1,
    )
    near_packed, outgoing, share = lax.optimization_barrier((near_packed, outgoing, share))
    other_packed = lax.ppermute(near_packed, "core", [(0, 1), (1, 0)])
    received = lax.all_to_all(
        outgoing.reshape(experts, capacity, -1), EP, split_axis=0, concat_axis=0, tiled=True
    )
    core = lax.axis_index("core").astype(jnp.int32).reshape(1)
    results, residual = expert(
        core,
        received.reshape(experts * capacity, -1),
        head_out,
        tokens,
        moe_gain,
        near_packed,
        other_packed,
        gate_weight,
        up_weight,
        down_weight,
    )
    returned = lax.all_to_all(
        results.reshape(experts, capacity, -1), EP, split_axis=0, concat_axis=0, tiled=True
    )
    return combine(share, returned.reshape(experts * capacity, -1), residual)


def solution(mesh):
    devices = mesh.devices.reshape(mesh.shape["grp"], -1, 4, 2)
    torus = Mesh(devices, ("grp", "far", "near", "core"))
    return jax.shard_map(
        local,
        mesh=torus,
        in_specs=(
            P(GRP_EP, None),
            P(),
            P(None, EP),
            P(),
            P(),
            P(None, EP),
            P(),
            P(),
            P(GRP_EP, None, None, None),
            P(GRP_EP, None, None, None),
            P(GRP_EP),
            P(),
            P(EP, None, None),
            P(EP, None, None),
            P(EP, None, None),
            P(GRP_EP, None),
            P(GRP_EP, None),
        ),
        out_specs=P(GRP_EP, None),
        check_vma=False,
    )
```

```python
import functools

import jax
import jax.numpy as jnp
from jax import lax
from jax.experimental import pallas as pl
from jax.experimental.pallas import tpu as pltpu
from jax.sharding import Mesh
from jax.sharding import PartitionSpec as P


EP = ("far", "near", "core")
NEAR = ("near", "core")
CHIPS = ("far", "near")
GRP_EP = ("grp", "far", "near", "core")


epsilon = 1e-06
masked_score = -1e30
clamp_limit = 7.0
swish_alpha = 1.702


def rms_scaled(values, gain):
    floats = values.astype(jnp.float32)
    return (
        floats
        * lax.rsqrt(jnp.mean(floats * floats, axis=-1, keepdims=True) + epsilon)
        * gain.astype(jnp.float32)
    )


def far_blocks(block):
    size = lax.axis_size("far")
    out = [block]
    for d in range(1, size):
        out.append(lax.ppermute(block, "far", [(i, (i + d) % size) for i in range(size)]))
    return out


def near_product(rows, blocks):
    members = lax.axis_size(NEAR)
    size = len(blocks)
    here = lax.axis_index("far")
    cols = blocks[0].shape[1]
    count = rows.shape[0] // members
    parts = [
        jnp.dot(rows, block, preferred_element_type=jnp.float32).astype(jnp.bfloat16)
        for block in blocks
    ]
    stacked = jnp.stack(parts[::-1] + parts[::-1])
    placed = lax.dynamic_slice_in_dim(stacked, size - 1 - here, size, axis=0)
    outgoing = jnp.transpose(placed.reshape(size, members, count, cols), (1, 2, 0, 3))
    return lax.all_to_all(
        outgoing.reshape(members, count, size * cols), NEAR, 0, 0, tiled=True
    )


def rows_of(ref):
    return jnp.concatenate([ref[i] for i in range(ref.shape[0])], axis=0)


def put_rows(ref, lanes, value):
    per = ref.shape[1]
    for i in range(ref.shape[0]):
        ref[i, :, lanes] = value[i * per : (i + 1) * per]


def attention_kernel(
    group_size, chunk, shard, lens_ref, lam_ref, r_ref, nk_ref, nv_ref, gain_ref, disp_ref, k_hbm, v_hbm,
    o_ref, out_ref, k_buf, v_buf, s_buf, q_buf, k_sem, v_sem,
):
    count, heads, width = q_buf.shape
    kv_count = nk_ref.shape[1] // width
    group = heads // kv_count
    half = width // 2
    rows = k_buf.shape[1]
    chunk_rows = chunk * kv_count
    chunks = rows // chunk_rows
    inv_scale = half ** (-0.5)
    channels = shard
    far_heads = width // channels

    def piece(c):
        return pl.ds(pl.multiple_of(c * chunk_rows, chunk_rows), chunk_rows)

    def copies(s, where):
        return (
            pltpu.make_async_copy(k_hbm.at[s, where], k_buf.at[s, where], k_sem.at[s]),
            pltpu.make_async_copy(v_hbm.at[s, where], v_buf.at[s, where], v_sem.at[s]),
        )

    def used(s):
        return (lens_ref[s] + chunk - 1) // chunk

    def fetch(s, _):
        n = used(s)
        for c in range(chunks):
            where = pl.ds(c * chunk_rows, chunk_rows)

            @pl.when(c < n)
            def _():
                for copy in copies(s, where):
                    copy.start()

            @pl.when(c >= n)
            def _():
                v_buf[s, where] = jnp.zeros((chunk_rows, width), v_buf.dtype)

        return 0

    lax.fori_loop(0, count, fetch, 0)

    for h in range(heads):
        parts = []
        for m in range(far_heads):
            piece_at = (h * far_heads + m) // r_ref.shape[0] * channels
            parts.append(
                r_ref[(h * far_heads + m) % r_ref.shape[0]].astype(jnp.float32)[
                    :, piece_at : piece_at + channels
                ]
            )
        q_buf[:, h, :] = jnp.concatenate(parts, axis=1)

    lane = lax.broadcasted_iota(jnp.int32, (heads, width), 1)
    head_row = lax.broadcasted_iota(jnp.int32, (heads, width), 0)
    column = lax.broadcasted_iota(jnp.int32, (1, heads, rows), 2)
    score_head = lax.broadcasted_iota(jnp.int32, (1, heads, rows), 1)
    own_kv = (column % kv_count) == score_head // group
    position = jnp.where(own_kv, column // kv_count, rows)[None]
    gain = gain_ref[...].astype(jnp.float32)
    lam = jnp.zeros((heads, 1), jnp.float32)
    for h in range(heads):
        lam = jnp.where(head_row[:, :1] == h, lam_ref[h], lam)
    lam = lam[None]
    low = (lane < half)[None]
    block = lax.broadcasted_iota(jnp.int32, (group_size, 1, heads, 1), 0)

    def spread(values):
        out = jnp.zeros((group_size, heads, width), jnp.float32)
        for k in range(kv_count):
            part = values[:, k * width : (k + 1) * width].reshape(group_size, 1, width)
            out = jnp.where((head_row // group == k)[None], part, out)
        return out

    def step(g, _):
        first = g * group_size
        here = pl.ds(first, group_size)
        q = q_buf[here].astype(jnp.bfloat16)
        zero = jnp.zeros_like(q)
        split = jnp.stack([jnp.where(low, q, zero), jnp.where(low, zero, q)], axis=1)
        own_key = spread(nk_ref[here].astype(jnp.float32))
        own_val = spread(nv_ref[here].astype(jnp.float32))
        own_score = (
            jnp.sum(split.astype(jnp.float32) * own_key[:, None], axis=3, keepdims=True) * inv_scale
        )
        limit = jnp.zeros((group_size, 1, heads, 1), jnp.int32)
        for i in range(group_size):
            s = first + i
            limit = jnp.where(block == i, lens_ref[s], limit)

            def wait(c, _):
                for copy in copies(s, piece(c)):
                    copy.wait()
                return 0

            lax.fori_loop(0, used(s), wait, 0)
        for i in range(group_size):
            s_buf[i] = lax.dot_general(
                split[i].reshape(2 * heads, width), k_buf[first + i], (((1,), (1,)), ((), ())), preferred_element_type=jnp.float32
            ).reshape(2, heads, rows)
        scores = jnp.where(position < limit, s_buf[...] * inv_scale, masked_score)
        highest = jnp.maximum(jnp.max(scores, axis=3, keepdims=True), own_score)
        expd = jnp.exp(scores - highest)
        own_exp = jnp.exp(own_score - highest)
        inverse = 1.0 / (jnp.sum(expd, axis=3, keepdims=True) + own_exp)
        plus = inverse[:, 0]
        minus = inverse[:, 1] * lam
        weights = (expd[:, 0] * plus - expd[:, 1] * minus).astype(jnp.bfloat16)
        own_weight = (own_exp[:, 0] * plus - own_exp[:, 1] * minus).astype(jnp.bfloat16)
        attended = jnp.stack(
            [
                jnp.dot(weights[i], v_buf[first + i], preferred_element_type=jnp.float32)
                for i in range(group_size)
            ]
        )
        attended = attended + own_weight.astype(jnp.float32) * own_val
        scale = lax.rsqrt(jnp.mean(attended * attended, axis=2, keepdims=True) + epsilon)
        q_buf[here] = (attended * scale * gain[None]).astype(o_ref.dtype).astype(jnp.float32)
        return 0

    lax.fori_loop(0, count // group_size, step, 0)
    heads_out = jnp.concatenate([q_buf[:, h, :] for h in range(heads)], axis=1).astype(o_ref.dtype)
    o_ref[...] = heads_out
    chosen = disp_ref[...]
    full = jnp.concatenate(
        [heads_out, jnp.zeros((chosen.shape[1] - count, heads * width), o_ref.dtype)], axis=0
    )
    put_rows(
        out_ref,
        pl.ds(0, heads * width),
        jnp.dot(chosen, full, preferred_element_type=jnp.float32).astype(out_ref.dtype),
    )
    put_rows(out_ref, pl.ds(heads * width, chosen.shape[1]), chosen)


def attention(
    queries, new_keys, new_values, cache_keys, cache_values, lengths, lambdas, head_gain, dispatch, experts
):
    count, ctx_len, kv_count, width = cache_keys.shape
    heads = lambdas.shape[0]
    slots, lanes = dispatch.shape
    shard = heads * width // experts
    vmem = pl.BlockSpec(memory_space=pltpu.VMEM)
    smem = pl.BlockSpec(memory_space=pltpu.SMEM)
    hbm = pl.BlockSpec(memory_space=pltpu.HBM)
    rows = ctx_len * kv_count
    together = 8
    return pl.pallas_call(
        functools.partial(attention_kernel, together, 128, shard),
        out_shape=(
            jax.ShapeDtypeStruct((count, heads * width), jnp.bfloat16),
            jax.ShapeDtypeStruct((experts, slots // experts, heads * width + lanes), jnp.bfloat16),
        ),
        in_specs=[smem, smem, vmem, vmem, vmem, vmem, vmem, hbm, hbm],
        out_specs=(vmem, vmem),
        scratch_shapes=[
            pltpu.VMEM((count, rows, width), jnp.bfloat16),
            pltpu.VMEM((count, rows, width), jnp.bfloat16),
            pltpu.VMEM((together, 2, heads, rows), jnp.float32),
            pltpu.VMEM((count, heads, width), jnp.float32),
            pltpu.SemaphoreType.DMA((count,)),
            pltpu.SemaphoreType.DMA((count,)),
        ],
        compiler_params=pltpu.CompilerParams(vmem_limit_bytes=56 * 2**20),
        name="attention",
    )(
        lengths,
        lambdas,
        queries,
        new_keys,
        new_values,
        head_gain.reshape(1, width),
        dispatch,
        cache_keys.reshape(count, rows, width),
        cache_values.reshape(count, rows, width),
    )


def expert_kernel(
    core_ref, h_ref, own_ref, tok_ref, gain_ref, near_hbm, other_hbm, gate_hbm, up_hbm, down_hbm,
    o_ref, res_ref, wo_buf, x_buf, gate_buf, up_buf, down_buf, wo_sem, x_sem, gate_sem, up_sem, down_sem,
):
    core = core_ref[0]
    cols = wo_buf.shape[1] // 2
    depth = wo_buf.shape[2]
    count = own_ref.shape[0]
    slots = h_ref.shape[0] * h_ref.shape[1]
    members = x_buf.shape[1] * 2
    halves = x_buf.shape[0]
    pieces = down_sem.shape[0]
    width = o_ref.shape[2]
    step = width // pieces

    wo_copies = []
    x_copies = []
    for i, source in enumerate((near_hbm, other_hbm)):
        side = core if i == 0 else 1 - core
        at = pl.ds(pl.multiple_of(side * cols, cols), cols)
        wo_copies.append(
            pltpu.make_async_copy(source.at[:, pl.ds(0, cols)], wo_buf.at[:, at], wo_sem.at[i])
        )
        at = pl.ds(pl.multiple_of(side * count, count), count)
        for half in range(halves):
            rows = pl.ds(cols + half * count, count)
            x_copies.append(
                pltpu.make_async_copy(
                    source.at[:, rows], x_buf.at[half, :, at], x_sem.at[i * halves + half]
                )
            )
    gate_copy = pltpu.make_async_copy(gate_hbm.at[0], gate_buf, gate_sem)
    up_copy = pltpu.make_async_copy(up_hbm.at[0], up_buf, up_sem)
    down_copies = [
        pltpu.make_async_copy(
            down_hbm.at[0, :, pl.ds(i * step, step)], down_buf.at[:, pl.ds(i * step, step)], down_sem.at[i]
        )
        for i in range(pieces)
    ]
    for copy in (*wo_copies, *x_copies, gate_copy, up_copy, *down_copies):
        copy.start()

    arrived = rows_of(h_ref)
    heads = jnp.concatenate([arrived[:, :depth], own_ref[...]], axis=0)
    chosen = arrived[:, depth:]
    lanes = chosen.shape[1]
    per = slots // members
    token = lax.broadcasted_iota(jnp.int32, (lanes, members * count), 0)
    column = lax.broadcasted_iota(jnp.int32, (lanes, members * count), 1)
    repeat = jnp.where(column % count == token, 1.0, 0.0).astype(jnp.bfloat16)
    spread = jnp.dot(chosen, repeat, preferred_element_type=jnp.float32)
    slot = lax.broadcasted_iota(jnp.int32, (slots, members * count), 0)
    column = lax.broadcasted_iota(jnp.int32, (slots, members * count), 1)
    select = jnp.where(slot // per == column // count, spread, 0.0).astype(jnp.bfloat16)

    for copy in wo_copies:
        copy.wait()
    attn = lax.dot_general(
        heads,
        wo_buf[...].reshape(width, depth),
        (((1,), (1,)), ((), ())),
        preferred_element_type=jnp.float32,
    ).astype(jnp.bfloat16)
    res_ref[...] = (
        tok_ref[...].astype(jnp.float32) + attn[slots:].astype(jnp.float32)
    ).astype(res_ref.dtype)
    for copy in x_copies:
        copy.wait()
    rows = jnp.concatenate(
        [
            jnp.dot(
                select,
                x_buf[half].reshape(members * count, depth),
                preferred_element_type=jnp.float32,
            )
            for half in range(halves)
        ],
        axis=1,
    )
    residual = (rows + attn[:slots].astype(jnp.float32)).astype(jnp.bfloat16)
    inputs = rms_scaled(residual, gain_ref[...]).astype(jnp.bfloat16)
    gate_copy.wait()
    gate = jnp.dot(inputs, gate_buf[...], preferred_element_type=jnp.float32)
    gate = jnp.minimum(gate, clamp_limit)
    swish = gate * (1.0 / (1.0 + jnp.exp(-swish_alpha * gate)))
    up_copy.wait()
    upper = jnp.dot(inputs, up_buf[...], preferred_element_type=jnp.float32)
    upper = jnp.clip(upper, -clamp_limit, clamp_limit)
    act = ((upper + 1.0) * swish).astype(jnp.bfloat16)
    for i, copy in enumerate(down_copies):
        copy.wait()
        at = pl.ds(i * step, step)
        put_rows(
            o_ref,
            at,
            jnp.dot(act, down_buf[:, at], preferred_element_type=jnp.float32).astype(o_ref.dtype),
        )


def expert(core, received, head_out, tokens, moe_gain, near, other, gate_w, up_w, down_w):
    members, per, _ = received.shape
    count, width = tokens.shape
    chips, packed, depth = near.shape
    halves = width // depth
    cols = packed - halves * count
    hidden = gate_w.shape[2]
    pieces = 4
    vmem = pl.BlockSpec(memory_space=pltpu.VMEM)
    smem = pl.BlockSpec(memory_space=pltpu.SMEM)
    hbm = pl.BlockSpec(memory_space=pltpu.HBM)
    bf16 = jnp.bfloat16
    return pl.pallas_call(
        expert_kernel,
        out_shape=(
            jax.ShapeDtypeStruct((members, per, width), bf16),
            jax.ShapeDtypeStruct((count, width), bf16),
        ),
        in_specs=[smem, vmem, vmem, vmem, vmem, hbm, hbm, hbm, hbm, hbm],
        out_specs=(vmem, vmem),
        scratch_shapes=[
            pltpu.VMEM((chips, 2 * cols, depth), bf16),
            pltpu.VMEM((halves, chips, 2 * count, depth), bf16),
            pltpu.VMEM((width, hidden), bf16),
            pltpu.VMEM((width, hidden), bf16),
            pltpu.VMEM((hidden, width), bf16),
            pltpu.SemaphoreType.DMA((2,)),
            pltpu.SemaphoreType.DMA((2 * halves,)),
            pltpu.SemaphoreType.DMA,
            pltpu.SemaphoreType.DMA,
            pltpu.SemaphoreType.DMA((pieces,)),
        ],
        compiler_params=pltpu.CompilerParams(vmem_limit_bytes=60 * 2**20),
        name="expert",
    )(core, received, head_out, tokens, moe_gain.reshape(1, width), near, other, gate_w, up_w, down_w)


def combine_kernel(share_ref, rows_ref, res_ref, o_ref):
    share = share_ref[...]
    high = share.astype(jnp.bfloat16)
    low = (share - high.astype(jnp.float32)).astype(jnp.bfloat16)
    rows = rows_of(rows_ref)
    total = jnp.dot(high, rows, preferred_element_type=jnp.float32) + jnp.dot(
        low, rows, preferred_element_type=jnp.float32
    )
    o_ref[...] = (res_ref[...].astype(jnp.float32) + total).astype(o_ref.dtype)


def combine(share, rows, residual):
    vmem = pl.BlockSpec(memory_space=pltpu.VMEM)
    return pl.pallas_call(
        combine_kernel,
        out_shape=jax.ShapeDtypeStruct(residual.shape, jnp.bfloat16),
        in_specs=[vmem] * 3,
        out_specs=vmem,
        compiler_params=pltpu.CompilerParams(vmem_limit_bytes=32 * 2**20),
        name="combine",
    )(share, rows, residual)


def local(
    tokens,
    norm_gain,
    query_weight,
    key_weight,
    value_weight,
    out_weight,
    head_gain,
    lambdas,
    cache_keys,
    cache_values,
    lengths,
    moe_gain,
    gate_weight,
    up_weight,
    down_weight,
    routes,
    route_weights,
):
    count = tokens.shape[0]
    topk = routes.shape[1]
    depth = out_weight.shape[0]
    packed = jnp.concatenate([out_weight.T, tokens[:, :depth], tokens[:, depth:]], axis=0)
    near_packed = lax.all_gather(packed, CHIPS, axis=0)
    query_blocks = far_blocks(query_weight)
    normed = rms_scaled(tokens, norm_gain).astype(jnp.bfloat16)
    new_keys = jnp.dot(normed, key_weight, preferred_element_type=jnp.float32).astype(jnp.bfloat16)
    new_values = jnp.dot(normed, value_weight, preferred_element_type=jnp.float32).astype(
        jnp.bfloat16
    )
    near_normed = lax.all_gather(normed, NEAR, axis=0, tiled=True)
    queries = near_product(near_normed, query_blocks)
    experts = lax.axis_size(EP)
    capacity = min(count, max(2, 2 * count * topk // experts))
    onehot = (routes.reshape(-1)[:, None] == jnp.arange(experts, dtype=jnp.int32)[None, :]).astype(
        jnp.int32
    )
    earlier_all = jnp.cumsum(onehot, axis=0) - onehot
    ranks = jnp.sum(earlier_all * onehot, axis=1).reshape(count, topk)
    slot_id = routes * capacity + ranks
    slot_range = jnp.arange(experts * capacity, dtype=jnp.int32)
    dispatch = jnp.any(slot_id[None, :, :] == slot_range[:, None, None], axis=2).astype(
        jnp.bfloat16
    )
    share = jnp.sum(
        jnp.where(slot_id[:, :, None] == slot_range[None, None, :], route_weights[:, :, None], 0.0),
        axis=1,
    )
    dispatch = jnp.pad(dispatch, ((0, 0), (0, 128 - count)))
    head_out, outgoing = attention(
        queries, new_keys, new_values, cache_keys, cache_values, lengths, lambdas, head_gain, dispatch, experts
    )
    received = lax.all_to_all(outgoing, EP, split_axis=0, concat_axis=0, tiled=True)
    near_packed, head_out = lax.optimization_barrier((near_packed, head_out))
    other_packed = lax.ppermute(near_packed, "core", [(0, 1), (1, 0)])
    core = lax.axis_index("core").astype(jnp.int32).reshape(1)
    results, residual = expert(
        core,
        received,
        head_out,
        tokens,
        moe_gain,
        near_packed,
        other_packed,
        gate_weight,
        up_weight,
        down_weight,
    )
    returned = lax.all_to_all(results, EP, split_axis=0, concat_axis=0, tiled=True)
    return combine(share, returned, residual)


def solution(mesh):
    devices = mesh.devices.reshape(mesh.shape["grp"], -1, 4, 2)
    torus = Mesh(devices, ("grp", "far", "near", "core"))
    return jax.shard_map(
        local,
        mesh=torus,
        in_specs=(
            P(GRP_EP, None),
            P(),
            P(None, EP),
            P(),
            P(),
            P(None, EP),
            P(),
            P(),
            P(GRP_EP, None, None, None),
            P(GRP_EP, None, None, None),
            P(GRP_EP),
            P(),
            P(EP, None, None),
            P(EP, None, None),
            P(EP, None, None),
            P(GRP_EP, None),
            P(GRP_EP, None),
        ),
        out_specs=P(GRP_EP, None),
        check_vma=False,
    )
```

```python
import functools

import jax
import jax.numpy as jnp
from jax import lax
from jax.experimental import pallas as pl
from jax.experimental.pallas import tpu as pltpu
from jax.sharding import Mesh
from jax.sharding import PartitionSpec as P


EP = ("far", "near", "core")
NEAR = ("near", "core")
CHIPS = ("far", "near")
GRP_EP = ("grp", "far", "near", "core")


epsilon = 1e-06
masked_score = -1e30
clamp_limit = 7.0
swish_alpha = 1.702


def rms_scaled(values, gain):
    floats = values.astype(jnp.float32)
    return (
        floats
        * lax.rsqrt(jnp.mean(floats * floats, axis=-1, keepdims=True) + epsilon)
        * gain.astype(jnp.float32)
    )


def query_exchange(normed, query_weight):
    members = lax.axis_size(NEAR)
    blocks = [query_weight.T]
    for d in range(1, members):
        blocks.append(lax.ppermute(query_weight.T, NEAR, [(i, i ^ d) for i in range(members)]))
    rows = lax.all_gather(normed, "far", axis=0, tiled=True)
    held = jnp.concatenate(blocks, axis=0)
    part = lax.dot_general(
        rows, held, (((1,), (1,)), ((), ())), preferred_element_type=jnp.float32
    ).astype(jnp.bfloat16)
    return lax.all_to_all(
        part.reshape(lax.axis_size("far"), normed.shape[0], held.shape[0]), "far", 0, 0, tiled=True
    )


def rows_of(ref):
    return jnp.concatenate([ref[i] for i in range(ref.shape[0])], axis=0)


def put_rows(ref, lanes, value):
    per = ref.shape[1]
    for i in range(ref.shape[0]):
        ref[i, :, lanes] = value[i * per : (i + 1) * per]


def attention_kernel(
    group_size, chunk, shard, member_ref, lens_ref, lam_ref, r_ref, nk_ref, nv_ref, gain_ref, disp_ref, k_hbm, v_hbm,
    o_ref, out_ref, k_buf, v_buf, s_buf, q_buf, k_sem, v_sem,
):
    count, heads, width = q_buf.shape
    kv_count = nk_ref.shape[1] // width
    group = heads // kv_count
    half = width // 2
    rows = k_buf.shape[1]
    chunk_rows = chunk * kv_count
    chunks = rows // chunk_rows
    inv_scale = half ** (-0.5)

    def piece(c):
        return pl.ds(pl.multiple_of(c * chunk_rows, chunk_rows), chunk_rows)

    def copies(s, where):
        return (
            pltpu.make_async_copy(k_hbm.at[s, where], k_buf.at[s, where], k_sem.at[s]),
            pltpu.make_async_copy(v_hbm.at[s, where], v_buf.at[s, where], v_sem.at[s]),
        )

    def used(s):
        return (lens_ref[s] + chunk - 1) // chunk

    def fetch(s, _):
        n = used(s)
        for c in range(chunks):
            where = pl.ds(c * chunk_rows, chunk_rows)

            @pl.when(c < n)
            def _():
                for copy in copies(s, where):
                    copy.start()

            @pl.when(c >= n)
            def _():
                v_buf[s, where] = jnp.zeros((chunk_rows, width), v_buf.dtype)

        return 0

    lax.fori_loop(0, count, fetch, 0)

    member = member_ref[0]
    place = lax.broadcasted_iota(jnp.int32, (count, width), 1) // shard
    for h in range(heads):
        head = r_ref[h].astype(jnp.float32)
        bit = 1
        while bit * shard < width:
            turned = jnp.where(
                (place // bit) % 2 == 0,
                pltpu.roll(head, width - bit * shard, 1),
                pltpu.roll(head, bit * shard, 1),
            )
            head = jnp.where((member // bit) % 2 == 1, turned, head)
            bit *= 2
        q_buf[:, h, :] = head

    lane = lax.broadcasted_iota(jnp.int32, (heads, width), 1)
    head_row = lax.broadcasted_iota(jnp.int32, (heads, width), 0)
    column = lax.broadcasted_iota(jnp.int32, (1, heads, rows), 2)
    score_head = lax.broadcasted_iota(jnp.int32, (1, heads, rows), 1)
    own_kv = (column % kv_count) == score_head // group
    position = jnp.where(own_kv, column // kv_count, rows)[None]
    gain = gain_ref[...].astype(jnp.float32)
    lam = jnp.zeros((heads, 1), jnp.float32)
    for h in range(heads):
        lam = jnp.where(head_row[:, :1] == h, lam_ref[h], lam)
    lam = lam[None]
    low = (lane < half)[None]
    block = lax.broadcasted_iota(jnp.int32, (group_size, 1, heads, 1), 0)

    def spread(values):
        out = jnp.zeros((group_size, heads, width), jnp.float32)
        for k in range(kv_count):
            part = values[:, k * width : (k + 1) * width].reshape(group_size, 1, width)
            out = jnp.where((head_row // group == k)[None], part, out)
        return out

    def step(g, _):
        first = g * group_size
        here = pl.ds(first, group_size)
        q = q_buf[here].astype(jnp.bfloat16)
        zero = jnp.zeros_like(q)
        split = jnp.stack([jnp.where(low, q, zero), jnp.where(low, zero, q)], axis=1)
        own_key = spread(nk_ref[here].astype(jnp.float32))
        own_val = spread(nv_ref[here].astype(jnp.float32))
        own_score = (
            jnp.sum(split.astype(jnp.float32) * own_key[:, None], axis=3, keepdims=True) * inv_scale
        )
        limit = jnp.zeros((group_size, 1, heads, 1), jnp.int32)
        for i in range(group_size):
            s = first + i
            limit = jnp.where(block == i, lens_ref[s], limit)

            def wait(c, _):
                for copy in copies(s, piece(c)):
                    copy.wait()
                return 0

            lax.fori_loop(0, used(s), wait, 0)
        for i in range(group_size):
            s_buf[i] = lax.dot_general(
                split[i].reshape(2 * heads, width), k_buf[first + i], (((1,), (1,)), ((), ())), preferred_element_type=jnp.float32
            ).reshape(2, heads, rows)
        scores = jnp.where(position < limit, s_buf[...] * inv_scale, masked_score)
        highest = jnp.maximum(jnp.max(scores, axis=3, keepdims=True), own_score)
        expd = jnp.exp(scores - highest)
        own_exp = jnp.exp(own_score - highest)
        inverse = 1.0 / (jnp.sum(expd, axis=3, keepdims=True) + own_exp)
        plus = inverse[:, 0]
        minus = inverse[:, 1] * lam
        weights = (expd[:, 0] * plus - expd[:, 1] * minus).astype(jnp.bfloat16)
        own_weight = (own_exp[:, 0] * plus - own_exp[:, 1] * minus).astype(jnp.bfloat16)
        attended = jnp.stack(
            [
                jnp.dot(weights[i], v_buf[first + i], preferred_element_type=jnp.float32)
                for i in range(group_size)
            ]
        )
        attended = attended + own_weight.astype(jnp.float32) * own_val
        scale = lax.rsqrt(jnp.mean(attended * attended, axis=2, keepdims=True) + epsilon)
        q_buf[here] = (attended * scale * gain[None]).astype(o_ref.dtype).astype(jnp.float32)
        return 0

    lax.fori_loop(0, count // group_size, step, 0)
    heads_out = jnp.concatenate([q_buf[:, h, :] for h in range(heads)], axis=1).astype(o_ref.dtype)
    o_ref[...] = heads_out
    chosen = disp_ref[...]
    full = jnp.concatenate(
        [heads_out, jnp.zeros((chosen.shape[1] - count, heads * width), o_ref.dtype)], axis=0
    )
    put_rows(
        out_ref,
        pl.ds(0, heads * width),
        jnp.dot(chosen, full, preferred_element_type=jnp.float32).astype(out_ref.dtype),
    )
    put_rows(out_ref, pl.ds(heads * width, chosen.shape[1]), chosen)


def attention(
    queries, new_keys, new_values, cache_keys, cache_values, lengths, lambdas, head_gain, dispatch, experts
):
    count, ctx_len, kv_count, width = cache_keys.shape
    heads = lambdas.shape[0]
    slots, lanes = dispatch.shape
    shard = heads * width // experts
    vmem = pl.BlockSpec(memory_space=pltpu.VMEM)
    smem = pl.BlockSpec(memory_space=pltpu.SMEM)
    hbm = pl.BlockSpec(memory_space=pltpu.HBM)
    rows = ctx_len * kv_count
    together = 8
    return pl.pallas_call(
        functools.partial(attention_kernel, together, 128, shard),
        out_shape=(
            jax.ShapeDtypeStruct((count, heads * width), jnp.bfloat16),
            jax.ShapeDtypeStruct((experts, slots // experts, heads * width + lanes), jnp.bfloat16),
        ),
        in_specs=[smem, smem, smem, vmem, vmem, vmem, vmem, vmem, hbm, hbm],
        out_specs=(vmem, vmem),
        scratch_shapes=[
            pltpu.VMEM((count, rows, width), jnp.bfloat16),
            pltpu.VMEM((count, rows, width), jnp.bfloat16),
            pltpu.VMEM((together, 2, heads, rows), jnp.float32),
            pltpu.VMEM((count, heads, width), jnp.float32),
            pltpu.SemaphoreType.DMA((count,)),
            pltpu.SemaphoreType.DMA((count,)),
        ],
        compiler_params=pltpu.CompilerParams(vmem_limit_bytes=53 * 2**20),
        name="attention",
    )(
        lax.axis_index(NEAR).astype(jnp.int32).reshape(1),
        lengths,
        lambdas,
        queries,
        new_keys,
        new_values,
        head_gain.reshape(1, width),
        dispatch,
        cache_keys.reshape(count, rows, width),
        cache_values.reshape(count, rows, width),
    )


def expert_kernel(
    core_ref, h_ref, own_ref, tok_ref, gain_ref, near_hbm, other_hbm, gate_hbm, up_hbm, down_hbm,
    o_ref, res_ref, wo_buf, x_buf, gate_buf, up_buf, down_buf, wo_sem, x_sem, gate_sem, up_sem, down_sem,
):
    core = core_ref[0]
    cols = wo_buf.shape[1] // 2
    depth = wo_buf.shape[2]
    count = own_ref.shape[0]
    slots = h_ref.shape[0] * h_ref.shape[1]
    members = x_buf.shape[1] * 2
    halves = x_buf.shape[0]
    pieces = down_sem.shape[0]
    width = o_ref.shape[2]
    step = width // pieces

    wo_copies = []
    x_copies = []
    for i, source in enumerate((near_hbm, other_hbm)):
        side = core if i == 0 else 1 - core
        at = pl.ds(pl.multiple_of(side * cols, cols), cols)
        wo_copies.append(
            pltpu.make_async_copy(source.at[:, pl.ds(0, cols)], wo_buf.at[:, at], wo_sem.at[i])
        )
        at = pl.ds(pl.multiple_of(side * count, count), count)
        for half in range(halves):
            rows = pl.ds(cols + half * count, count)
            x_copies.append(
                pltpu.make_async_copy(
                    source.at[:, rows], x_buf.at[half, :, at], x_sem.at[i * halves + half]
                )
            )
    gate_copy = pltpu.make_async_copy(gate_hbm.at[0], gate_buf, gate_sem)
    up_copy = pltpu.make_async_copy(up_hbm.at[0], up_buf, up_sem)
    down_copies = [
        pltpu.make_async_copy(
            down_hbm.at[0, :, pl.ds(i * step, step)], down_buf.at[:, pl.ds(i * step, step)], down_sem.at[i]
        )
        for i in range(pieces)
    ]
    for copy in (*wo_copies, *x_copies, gate_copy, up_copy, *down_copies):
        copy.start()

    arrived = rows_of(h_ref)
    heads = jnp.concatenate([arrived[:, :depth], own_ref[...]], axis=0)
    chosen = arrived[:, depth:]
    lanes = chosen.shape[1]
    per = slots // members
    token = lax.broadcasted_iota(jnp.int32, (lanes, members * count), 0)
    column = lax.broadcasted_iota(jnp.int32, (lanes, members * count), 1)
    repeat = jnp.where(column % count == token, 1.0, 0.0).astype(jnp.bfloat16)
    spread = jnp.dot(chosen, repeat, preferred_element_type=jnp.float32)
    slot = lax.broadcasted_iota(jnp.int32, (slots, members * count), 0)
    column = lax.broadcasted_iota(jnp.int32, (slots, members * count), 1)
    select = jnp.where(slot // per == column // count, spread, 0.0).astype(jnp.bfloat16)

    for copy in wo_copies:
        copy.wait()
    attn = lax.dot_general(
        heads,
        wo_buf[...].reshape(width, depth),
        (((1,), (1,)), ((), ())),
        preferred_element_type=jnp.float32,
    ).astype(jnp.bfloat16)
    res_ref[...] = (
        tok_ref[...].astype(jnp.float32) + attn[slots:].astype(jnp.float32)
    ).astype(res_ref.dtype)
    for copy in x_copies:
        copy.wait()
    rows = jnp.concatenate(
        [
            jnp.dot(
                select,
                x_buf[half].reshape(members * count, depth),
                preferred_element_type=jnp.float32,
            )
            for half in range(halves)
        ],
        axis=1,
    )
    residual = (rows + attn[:slots].astype(jnp.float32)).astype(jnp.bfloat16)
    inputs = rms_scaled(residual, gain_ref[...]).astype(jnp.bfloat16)
    gate_copy.wait()
    gate = jnp.dot(inputs, gate_buf[...], preferred_element_type=jnp.float32)
    gate = jnp.minimum(gate, clamp_limit)
    swish = gate * (1.0 / (1.0 + jnp.exp(-swish_alpha * gate)))
    up_copy.wait()
    upper = jnp.dot(inputs, up_buf[...], preferred_element_type=jnp.float32)
    upper = jnp.clip(upper, -clamp_limit, clamp_limit)
    act = ((upper + 1.0) * swish).astype(jnp.bfloat16)
    for i, copy in enumerate(down_copies):
        copy.wait()
        at = pl.ds(i * step, step)
        put_rows(
            o_ref,
            at,
            jnp.dot(act, down_buf[:, at], preferred_element_type=jnp.float32).astype(o_ref.dtype),
        )


def expert(core, received, head_out, tokens, moe_gain, near, other, gate_w, up_w, down_w):
    members, per, _ = received.shape
    count, width = tokens.shape
    chips, packed, depth = near.shape
    halves = width // depth
    cols = packed - halves * count
    hidden = gate_w.shape[2]
    pieces = 4
    vmem = pl.BlockSpec(memory_space=pltpu.VMEM)
    smem = pl.BlockSpec(memory_space=pltpu.SMEM)
    hbm = pl.BlockSpec(memory_space=pltpu.HBM)
    bf16 = jnp.bfloat16
    return pl.pallas_call(
        expert_kernel,
        out_shape=(
            jax.ShapeDtypeStruct((members, per, width), bf16),
            jax.ShapeDtypeStruct((count, width), bf16),
        ),
        in_specs=[smem, vmem, vmem, vmem, vmem, hbm, hbm, hbm, hbm, hbm],
        out_specs=(vmem, vmem),
        scratch_shapes=[
            pltpu.VMEM((chips, 2 * cols, depth), bf16),
            pltpu.VMEM((halves, chips, 2 * count, depth), bf16),
            pltpu.VMEM((width, hidden), bf16),
            pltpu.VMEM((width, hidden), bf16),
            pltpu.VMEM((hidden, width), bf16),
            pltpu.SemaphoreType.DMA((2,)),
            pltpu.SemaphoreType.DMA((2 * halves,)),
            pltpu.SemaphoreType.DMA,
            pltpu.SemaphoreType.DMA,
            pltpu.SemaphoreType.DMA((pieces,)),
        ],
        compiler_params=pltpu.CompilerParams(vmem_limit_bytes=50 * 2**20),
        name="expert",
    )(core, received, head_out, tokens, moe_gain.reshape(1, width), near, other, gate_w, up_w, down_w)


def combine_kernel(share_ref, rows_ref, res_ref, o_ref):
    share = share_ref[...]
    high = share.astype(jnp.bfloat16)
    low = (share - high.astype(jnp.float32)).astype(jnp.bfloat16)
    rows = rows_of(rows_ref)
    total = jnp.dot(high, rows, preferred_element_type=jnp.float32) + jnp.dot(
        low, rows, preferred_element_type=jnp.float32
    )
    o_ref[...] = (res_ref[...].astype(jnp.float32) + total).astype(o_ref.dtype)


def combine(share, rows, residual):
    vmem = pl.BlockSpec(memory_space=pltpu.VMEM)
    return pl.pallas_call(
        combine_kernel,
        out_shape=jax.ShapeDtypeStruct(residual.shape, jnp.bfloat16),
        in_specs=[vmem] * 3,
        out_specs=vmem,
        compiler_params=pltpu.CompilerParams(vmem_limit_bytes=32 * 2**20),
        name="combine",
    )(share, rows, residual)


def local(
    tokens,
    norm_gain,
    query_weight,
    key_weight,
    value_weight,
    out_weight,
    head_gain,
    lambdas,
    cache_keys,
    cache_values,
    lengths,
    moe_gain,
    gate_weight,
    up_weight,
    down_weight,
    routes,
    route_weights,
):
    count = tokens.shape[0]
    topk = routes.shape[1]
    depth = out_weight.shape[0]
    packed = jnp.concatenate([out_weight.T, tokens[:, :depth], tokens[:, depth:]], axis=0)
    near_packed = lax.all_gather(packed, CHIPS, axis=0)
    normed = rms_scaled(tokens, norm_gain).astype(jnp.bfloat16)
    queries = query_exchange(normed, query_weight)
    new_keys = jnp.dot(normed, key_weight, preferred_element_type=jnp.float32).astype(jnp.bfloat16)
    new_values = jnp.dot(normed, value_weight, preferred_element_type=jnp.float32).astype(
        jnp.bfloat16
    )
    experts = lax.axis_size(EP)
    capacity = min(count, max(2, 2 * count * topk // experts))
    onehot = (routes.reshape(-1)[:, None] == jnp.arange(experts, dtype=jnp.int32)[None, :]).astype(
        jnp.int32
    )
    earlier_all = jnp.cumsum(onehot, axis=0) - onehot
    ranks = jnp.sum(earlier_all * onehot, axis=1).reshape(count, topk)
    slot_id = routes * capacity + ranks
    slot_range = jnp.arange(experts * capacity, dtype=jnp.int32)
    dispatch = jnp.any(slot_id[None, :, :] == slot_range[:, None, None], axis=2).astype(
        jnp.bfloat16
    )
    share = jnp.sum(
        jnp.where(slot_id[:, :, None] == slot_range[None, None, :], route_weights[:, :, None], 0.0),
        axis=1,
    )
    dispatch = jnp.pad(dispatch, ((0, 0), (0, 128 - count)))
    head_out, outgoing = attention(
        queries, new_keys, new_values, cache_keys, cache_values, lengths, lambdas, head_gain, dispatch, experts
    )
    received = lax.all_to_all(outgoing, EP, split_axis=0, concat_axis=0, tiled=True)
    near_packed, head_out = lax.optimization_barrier((near_packed, head_out))
    other_packed = lax.ppermute(near_packed, "core", [(0, 1), (1, 0)])
    core = lax.axis_index("core").astype(jnp.int32).reshape(1)
    results, residual = expert(
        core,
        received,
        head_out,
        tokens,
        moe_gain,
        near_packed,
        other_packed,
        gate_weight,
        up_weight,
        down_weight,
    )
    returned = lax.all_to_all(results, EP, split_axis=0, concat_axis=0, tiled=True)
    return combine(share, returned, residual)


def solution(mesh):
    devices = mesh.devices.reshape(mesh.shape["grp"], -1, 2, 2)
    torus = Mesh(devices, ("grp", "far", "near", "core"))
    return jax.shard_map(
        local,
        mesh=torus,
        in_specs=(
            P(GRP_EP, None),
            P(),
            P(None, EP),
            P(),
            P(),
            P(None, EP),
            P(),
            P(),
            P(GRP_EP, None, None, None),
            P(GRP_EP, None, None, None),
            P(GRP_EP),
            P(),
            P(EP, None, None),
            P(EP, None, None),
            P(EP, None, None),
            P(GRP_EP, None),
            P(GRP_EP, None),
        ),
        out_specs=P(GRP_EP, None),
        check_vma=False,
    )
```

```python
import functools

import jax
import jax.numpy as jnp
from jax import lax
from jax.experimental import pallas as pl
from jax.experimental.pallas import tpu as pltpu
from jax.sharding import Mesh
from jax.sharding import PartitionSpec as P


EP = ("far", "near", "core")
NEAR = ("near", "core")
CHIPS = ("far", "near")
GRP_EP = ("grp", "far", "near", "core")


epsilon = 1e-06
masked_score = -1e30
clamp_limit = 7.0
swish_alpha = 1.702


def rms_scaled(values, gain):
    floats = values.astype(jnp.float32)
    return (
        floats
        * lax.rsqrt(jnp.mean(floats * floats, axis=-1, keepdims=True) + epsilon)
        * gain.astype(jnp.float32)
    )


def query_kernel(place_ref, rows_ref, gain_ref, *refs):
    *block_refs, part_ref, own_ref = refs
    count = own_ref.shape[0]
    normed = rms_scaled(rows_ref[...], gain_ref[...]).astype(jnp.bfloat16)
    held = jnp.concatenate([ref[...] for ref in block_refs], axis=0)
    part = lax.dot_general(
        normed, held, (((1,), (1,)), ((), ())), preferred_element_type=jnp.float32
    ).astype(part_ref.dtype)
    own = rows_ref[pl.ds(pl.multiple_of(place_ref[0] * count, count), count)]
    own_ref[...] = rms_scaled(own, gain_ref[...]).astype(own_ref.dtype)
    for i in range(part_ref.shape[0]):
        part_ref[i] = part[i * count : (i + 1) * count]


def query_product(tokens, norm_gain, query_weight):
    count, width = tokens.shape
    members = lax.axis_size(NEAR)
    shard = query_weight.T
    blocks = [shard]
    for d in range(1, members):
        blocks.append(lax.ppermute(shard, NEAR, [(i, i ^ d) for i in range(members)]))
    rows = lax.all_gather(tokens, "far", axis=0, tiled=True)
    far = lax.axis_size("far")
    vmem = pl.BlockSpec(memory_space=pltpu.VMEM)
    smem = pl.BlockSpec(memory_space=pltpu.SMEM)
    return pl.pallas_call(
        query_kernel,
        out_shape=(
            jax.ShapeDtypeStruct((far, count, members * shard.shape[0]), jnp.bfloat16),
            jax.ShapeDtypeStruct((count, width), jnp.bfloat16),
        ),
        in_specs=[smem] + [vmem] * (2 + members),
        out_specs=(vmem, vmem),
        compiler_params=pltpu.CompilerParams(vmem_limit_bytes=50 * 2**20),
        name="query",
    )(
        lax.axis_index("far").astype(jnp.int32).reshape(1),
        rows,
        norm_gain.reshape(1, width),
        *blocks,
    )


def rows_of(ref):
    return jnp.concatenate([ref[i] for i in range(ref.shape[0])], axis=0)


def put_rows(ref, lanes, value):
    per = ref.shape[1]
    for i in range(ref.shape[0]):
        ref[i, :, lanes] = value[i * per : (i + 1) * per]


def attention_kernel(
    group_size, chunk, shard, member_ref, lens_ref, lam_ref, r_ref, nk_ref, nv_ref, gain_ref, disp_ref, k_hbm, v_hbm,
    o_ref, out_ref, k_buf, v_buf, s_buf, q_buf, k_sem, v_sem,
):
    count, heads, width = q_buf.shape
    kv_count = nk_ref.shape[1] // width
    group = heads // kv_count
    half = width // 2
    rows = k_buf.shape[1]
    chunk_rows = chunk * kv_count
    chunks = rows // chunk_rows
    inv_scale = half ** (-0.5)

    def piece(c):
        return pl.ds(pl.multiple_of(c * chunk_rows, chunk_rows), chunk_rows)

    def copies(s, where):
        return (
            pltpu.make_async_copy(k_hbm.at[s, where], k_buf.at[s, where], k_sem.at[s]),
            pltpu.make_async_copy(v_hbm.at[s, where], v_buf.at[s, where], v_sem.at[s]),
        )

    def used(s):
        return (lens_ref[s] + chunk - 1) // chunk

    def fetch(s, _):
        n = used(s)
        for c in range(chunks):
            where = pl.ds(c * chunk_rows, chunk_rows)

            @pl.when(c < n)
            def _():
                for copy in copies(s, where):
                    copy.start()

            @pl.when(c >= n)
            def _():
                v_buf[s, where] = jnp.zeros((chunk_rows, width), v_buf.dtype)

        return 0

    lax.fori_loop(0, count, fetch, 0)

    member = member_ref[0]
    place = lax.broadcasted_iota(jnp.int32, (count, width), 1) // shard
    for h in range(heads):
        head = r_ref[h].astype(jnp.float32)
        bit = 1
        while bit * shard < width:
            turned = jnp.where(
                (place // bit) % 2 == 0,
                pltpu.roll(head, width - bit * shard, 1),
                pltpu.roll(head, bit * shard, 1),
            )
            head = jnp.where((member // bit) % 2 == 1, turned, head)
            bit *= 2
        q_buf[:, h, :] = head

    lane = lax.broadcasted_iota(jnp.int32, (heads, width), 1)
    head_row = lax.broadcasted_iota(jnp.int32, (heads, width), 0)
    column = lax.broadcasted_iota(jnp.int32, (1, heads, rows), 2)
    score_head = lax.broadcasted_iota(jnp.int32, (1, heads, rows), 1)
    own_kv = (column % kv_count) == score_head // group
    position = jnp.where(own_kv, column // kv_count, rows)[None]
    gain = gain_ref[...].astype(jnp.float32)
    lam = jnp.zeros((heads, 1), jnp.float32)
    for h in range(heads):
        lam = jnp.where(head_row[:, :1] == h, lam_ref[h], lam)
    lam = lam[None]
    low = (lane < half)[None]
    block = lax.broadcasted_iota(jnp.int32, (group_size, 1, heads, 1), 0)

    def spread(values):
        out = jnp.zeros((group_size, heads, width), jnp.float32)
        for k in range(kv_count):
            part = values[:, k * width : (k + 1) * width].reshape(group_size, 1, width)
            out = jnp.where((head_row // group == k)[None], part, out)
        return out

    def step(g, _):
        first = g * group_size
        here = pl.ds(first, group_size)
        q = q_buf[here].astype(jnp.bfloat16)
        zero = jnp.zeros_like(q)
        split = jnp.stack([jnp.where(low, q, zero), jnp.where(low, zero, q)], axis=1)
        own_key = spread(nk_ref[here].astype(jnp.float32))
        own_val = spread(nv_ref[here].astype(jnp.float32))
        own_score = (
            jnp.sum(split.astype(jnp.float32) * own_key[:, None], axis=3, keepdims=True) * inv_scale
        )
        limit = jnp.zeros((group_size, 1, heads, 1), jnp.int32)
        for i in range(group_size):
            s = first + i
            limit = jnp.where(block == i, lens_ref[s], limit)

            def wait(c, _):
                for copy in copies(s, piece(c)):
                    copy.wait()
                return 0

            lax.fori_loop(0, used(s), wait, 0)
        for i in range(group_size):
            s_buf[i] = lax.dot_general(
                split[i].reshape(2 * heads, width), k_buf[first + i], (((1,), (1,)), ((), ())), preferred_element_type=jnp.float32
            ).reshape(2, heads, rows)
        scores = jnp.where(position < limit, s_buf[...] * inv_scale, masked_score)
        highest = jnp.maximum(jnp.max(scores, axis=3, keepdims=True), own_score)
        expd = jnp.exp(scores - highest)
        own_exp = jnp.exp(own_score - highest)
        inverse = 1.0 / (jnp.sum(expd, axis=3, keepdims=True) + own_exp)
        plus = inverse[:, 0]
        minus = inverse[:, 1] * lam
        weights = (expd[:, 0] * plus - expd[:, 1] * minus).astype(jnp.bfloat16)
        own_weight = (own_exp[:, 0] * plus - own_exp[:, 1] * minus).astype(jnp.bfloat16)
        attended = jnp.stack(
            [
                jnp.dot(weights[i], v_buf[first + i], preferred_element_type=jnp.float32)
                for i in range(group_size)
            ]
        )
        attended = attended + own_weight.astype(jnp.float32) * own_val
        scale = lax.rsqrt(jnp.mean(attended * attended, axis=2, keepdims=True) + epsilon)
        q_buf[here] = (attended * scale * gain[None]).astype(o_ref.dtype).astype(jnp.float32)
        return 0

    lax.fori_loop(0, count // group_size, step, 0)
    heads_out = jnp.concatenate([q_buf[:, h, :] for h in range(heads)], axis=1).astype(o_ref.dtype)
    o_ref[...] = heads_out
    chosen = disp_ref[...]
    full = jnp.concatenate(
        [heads_out, jnp.zeros((chosen.shape[1] - count, heads * width), o_ref.dtype)], axis=0
    )
    put_rows(
        out_ref,
        pl.ds(0, heads * width),
        jnp.dot(chosen, full, preferred_element_type=jnp.float32).astype(out_ref.dtype),
    )
    put_rows(out_ref, pl.ds(heads * width, chosen.shape[1]), chosen)


def attention(
    queries, new_keys, new_values, cache_keys, cache_values, lengths, lambdas, head_gain, dispatch, experts
):
    count, ctx_len, kv_count, width = cache_keys.shape
    heads = lambdas.shape[0]
    slots, lanes = dispatch.shape
    shard = heads * width // experts
    vmem = pl.BlockSpec(memory_space=pltpu.VMEM)
    smem = pl.BlockSpec(memory_space=pltpu.SMEM)
    hbm = pl.BlockSpec(memory_space=pltpu.HBM)
    rows = ctx_len * kv_count
    together = 8
    return pl.pallas_call(
        functools.partial(attention_kernel, together, 128, shard),
        out_shape=(
            jax.ShapeDtypeStruct((count, heads * width), jnp.bfloat16),
            jax.ShapeDtypeStruct((experts, slots // experts, heads * width + lanes), jnp.bfloat16),
        ),
        in_specs=[smem, smem, smem, vmem, vmem, vmem, vmem, vmem, hbm, hbm],
        out_specs=(vmem, vmem),
        scratch_shapes=[
            pltpu.VMEM((count, rows, width), jnp.bfloat16),
            pltpu.VMEM((count, rows, width), jnp.bfloat16),
            pltpu.VMEM((together, 2, heads, rows), jnp.float32),
            pltpu.VMEM((count, heads, width), jnp.float32),
            pltpu.SemaphoreType.DMA((count,)),
            pltpu.SemaphoreType.DMA((count,)),
        ],
        compiler_params=pltpu.CompilerParams(vmem_limit_bytes=53 * 2**20),
        name="attention",
    )(
        lax.axis_index(NEAR).astype(jnp.int32).reshape(1),
        lengths,
        lambdas,
        queries,
        new_keys,
        new_values,
        head_gain.reshape(1, width),
        dispatch,
        cache_keys.reshape(count, rows, width),
        cache_values.reshape(count, rows, width),
    )


def expert_kernel(
    core_ref, h_ref, own_ref, tok_ref, gain_ref, near_hbm, other_hbm, gate_hbm, up_hbm, down_hbm,
    o_ref, res_ref, wo_buf, x_buf, gate_buf, up_buf, down_buf, wo_sem, x_sem, gate_sem, up_sem, down_sem,
):
    core = core_ref[0]
    cols = wo_buf.shape[1] // 2
    depth = wo_buf.shape[2]
    count = own_ref.shape[0]
    slots = h_ref.shape[0] * h_ref.shape[1]
    members = x_buf.shape[1] * 2
    halves = x_buf.shape[0]
    pieces = down_sem.shape[0]
    width = o_ref.shape[2]
    step = width // pieces

    wo_copies = []
    x_copies = []
    for i, source in enumerate((near_hbm, other_hbm)):
        side = core if i == 0 else 1 - core
        at = pl.ds(pl.multiple_of(side * cols, cols), cols)
        wo_copies.append(
            pltpu.make_async_copy(source.at[:, pl.ds(0, cols)], wo_buf.at[:, at], wo_sem.at[i])
        )
        at = pl.ds(pl.multiple_of(side * count, count), count)
        for half in range(halves):
            rows = pl.ds(cols + half * count, count)
            x_copies.append(
                pltpu.make_async_copy(
                    source.at[:, rows], x_buf.at[half, :, at], x_sem.at[i * halves + half]
                )
            )
    gate_copy = pltpu.make_async_copy(gate_hbm.at[0], gate_buf, gate_sem)
    up_copy = pltpu.make_async_copy(up_hbm.at[0], up_buf, up_sem)
    down_copies = [
        pltpu.make_async_copy(
            down_hbm.at[0, :, pl.ds(i * step, step)], down_buf.at[:, pl.ds(i * step, step)], down_sem.at[i]
        )
        for i in range(pieces)
    ]
    for copy in (*wo_copies, *x_copies, gate_copy, up_copy, *down_copies):
        copy.start()

    arrived = rows_of(h_ref)
    heads = jnp.concatenate([arrived[:, :depth], own_ref[...]], axis=0)
    chosen = arrived[:, depth:]
    lanes = chosen.shape[1]
    per = slots // members
    token = lax.broadcasted_iota(jnp.int32, (lanes, members * count), 0)
    column = lax.broadcasted_iota(jnp.int32, (lanes, members * count), 1)
    repeat = jnp.where(column % count == token, 1.0, 0.0).astype(jnp.bfloat16)
    spread = jnp.dot(chosen, repeat, preferred_element_type=jnp.float32)
    slot = lax.broadcasted_iota(jnp.int32, (slots, members * count), 0)
    column = lax.broadcasted_iota(jnp.int32, (slots, members * count), 1)
    select = jnp.where(slot // per == column // count, spread, 0.0).astype(jnp.bfloat16)

    for copy in wo_copies:
        copy.wait()
    attn = lax.dot_general(
        heads,
        wo_buf[...].reshape(width, depth),
        (((1,), (1,)), ((), ())),
        preferred_element_type=jnp.float32,
    ).astype(jnp.bfloat16)
    res_ref[...] = (
        tok_ref[...].astype(jnp.float32) + attn[slots:].astype(jnp.float32)
    ).astype(res_ref.dtype)
    for copy in x_copies:
        copy.wait()
    rows = jnp.concatenate(
        [
            jnp.dot(
                select,
                x_buf[half].reshape(members * count, depth),
                preferred_element_type=jnp.float32,
            )
            for half in range(halves)
        ],
        axis=1,
    )
    residual = (rows + attn[:slots].astype(jnp.float32)).astype(jnp.bfloat16)
    inputs = rms_scaled(residual, gain_ref[...]).astype(jnp.bfloat16)
    gate_copy.wait()
    gate = jnp.dot(inputs, gate_buf[...], preferred_element_type=jnp.float32)
    gate = jnp.minimum(gate, clamp_limit)
    swish = gate * (1.0 / (1.0 + jnp.exp(-swish_alpha * gate)))
    up_copy.wait()
    upper = jnp.dot(inputs, up_buf[...], preferred_element_type=jnp.float32)
    upper = jnp.clip(upper, -clamp_limit, clamp_limit)
    act = ((upper + 1.0) * swish).astype(jnp.bfloat16)
    for i, copy in enumerate(down_copies):
        copy.wait()
        at = pl.ds(i * step, step)
        put_rows(
            o_ref,
            at,
            jnp.dot(act, down_buf[:, at], preferred_element_type=jnp.float32).astype(o_ref.dtype),
        )


def expert(core, received, head_out, tokens, moe_gain, near, other, gate_w, up_w, down_w):
    members, per, _ = received.shape
    count, width = tokens.shape
    chips, packed, depth = near.shape
    halves = width // depth
    cols = packed - halves * count
    hidden = gate_w.shape[2]
    pieces = 4
    vmem = pl.BlockSpec(memory_space=pltpu.VMEM)
    smem = pl.BlockSpec(memory_space=pltpu.SMEM)
    hbm = pl.BlockSpec(memory_space=pltpu.HBM)
    bf16 = jnp.bfloat16
    return pl.pallas_call(
        expert_kernel,
        out_shape=(
            jax.ShapeDtypeStruct((members, per, width), bf16),
            jax.ShapeDtypeStruct((count, width), bf16),
        ),
        in_specs=[smem, vmem, vmem, vmem, vmem, hbm, hbm, hbm, hbm, hbm],
        out_specs=(vmem, vmem),
        scratch_shapes=[
            pltpu.VMEM((chips, 2 * cols, depth), bf16),
            pltpu.VMEM((halves, chips, 2 * count, depth), bf16),
            pltpu.VMEM((width, hidden), bf16),
            pltpu.VMEM((width, hidden), bf16),
            pltpu.VMEM((hidden, width), bf16),
            pltpu.SemaphoreType.DMA((2,)),
            pltpu.SemaphoreType.DMA((2 * halves,)),
            pltpu.SemaphoreType.DMA,
            pltpu.SemaphoreType.DMA,
            pltpu.SemaphoreType.DMA((pieces,)),
        ],
        compiler_params=pltpu.CompilerParams(vmem_limit_bytes=50 * 2**20),
        name="expert",
    )(core, received, head_out, tokens, moe_gain.reshape(1, width), near, other, gate_w, up_w, down_w)


def combine_kernel(share_ref, rows_ref, res_ref, o_ref):
    share = share_ref[...]
    high = share.astype(jnp.bfloat16)
    low = (share - high.astype(jnp.float32)).astype(jnp.bfloat16)
    rows = rows_of(rows_ref)
    total = jnp.dot(high, rows, preferred_element_type=jnp.float32) + jnp.dot(
        low, rows, preferred_element_type=jnp.float32
    )
    o_ref[...] = (res_ref[...].astype(jnp.float32) + total).astype(o_ref.dtype)


def combine(share, rows, residual):
    vmem = pl.BlockSpec(memory_space=pltpu.VMEM)
    return pl.pallas_call(
        combine_kernel,
        out_shape=jax.ShapeDtypeStruct(residual.shape, jnp.bfloat16),
        in_specs=[vmem] * 3,
        out_specs=vmem,
        compiler_params=pltpu.CompilerParams(vmem_limit_bytes=32 * 2**20),
        name="combine",
    )(share, rows, residual)


def local(
    tokens,
    norm_gain,
    query_weight,
    key_weight,
    value_weight,
    out_weight,
    head_gain,
    lambdas,
    cache_keys,
    cache_values,
    lengths,
    moe_gain,
    gate_weight,
    up_weight,
    down_weight,
    routes,
    route_weights,
):
    count = tokens.shape[0]
    topk = routes.shape[1]
    depth = out_weight.shape[0]
    packed = jnp.concatenate([out_weight.T, tokens[:, :depth], tokens[:, depth:]], axis=0)
    near_packed = lax.all_gather(packed, CHIPS, axis=0)
    part, normed = query_product(tokens, norm_gain, query_weight)
    queries = lax.all_to_all(part, "far", 0, 0, tiled=True)
    new_keys = jnp.dot(normed, key_weight, preferred_element_type=jnp.float32).astype(jnp.bfloat16)
    new_values = jnp.dot(normed, value_weight, preferred_element_type=jnp.float32).astype(
        jnp.bfloat16
    )
    experts = lax.axis_size(EP)
    capacity = min(count, max(2, 2 * count * topk // experts))
    routes, new_keys = lax.optimization_barrier((routes, new_keys))
    slot_range = jnp.arange(experts * capacity, dtype=jnp.int32)
    onehot = (
        routes.reshape(-1)[:, None] == jnp.arange(experts, dtype=jnp.int32)[None, :]
    ).astype(jnp.int32)
    earlier_all = jnp.cumsum(onehot, axis=0) - onehot
    ranks = jnp.sum(earlier_all * onehot, axis=1).reshape(count, topk)
    slot_id = routes * capacity + ranks
    dispatch = jnp.any(slot_id[None, :, :] == slot_range[:, None, None], axis=2).astype(
        jnp.bfloat16
    )
    dispatch = jnp.pad(dispatch, ((0, 0), (0, 128 - count)))
    share = jnp.sum(
        jnp.where(slot_id[:, :, None] == slot_range[None, None, :], route_weights[:, :, None], 0.0),
        axis=1,
    )
    head_out, outgoing = attention(
        queries, new_keys, new_values, cache_keys, cache_values, lengths, lambdas, head_gain, dispatch, experts
    )
    received = lax.all_to_all(outgoing, EP, split_axis=0, concat_axis=0, tiled=True)
    near_packed, head_out = lax.optimization_barrier((near_packed, head_out))
    other_packed = lax.ppermute(near_packed, "core", [(0, 1), (1, 0)])
    core = lax.axis_index("core").astype(jnp.int32).reshape(1)
    results, residual = expert(
        core,
        received,
        head_out,
        tokens,
        moe_gain,
        near_packed,
        other_packed,
        gate_weight,
        up_weight,
        down_weight,
    )
    returned = lax.all_to_all(results, EP, split_axis=0, concat_axis=0, tiled=True)
    return combine(share, returned, residual)


def solution(mesh):
    devices = mesh.devices.reshape(mesh.shape["grp"], -1, 2, 2)
    torus = Mesh(devices, ("grp", "far", "near", "core"))
    return jax.shard_map(
        local,
        mesh=torus,
        in_specs=(
            P(GRP_EP, None),
            P(),
            P(None, EP),
            P(),
            P(),
            P(None, EP),
            P(),
            P(),
            P(GRP_EP, None, None, None),
            P(GRP_EP, None, None, None),
            P(GRP_EP),
            P(),
            P(EP, None, None),
            P(EP, None, None),
            P(EP, None, None),
            P(GRP_EP, None),
            P(GRP_EP, None),
        ),
        out_specs=P(GRP_EP, None),
        check_vma=False,
    )
```

```python
import functools

import jax
import jax.numpy as jnp
from jax import lax
from jax.experimental import pallas as pl
from jax.experimental.pallas import tpu as pltpu
from jax.sharding import Mesh
from jax.sharding import PartitionSpec as P


EP = ("far", "near", "core")
NEAR = ("near", "core")
CHIPS = ("far", "near")
GRP_EP = ("grp", "far", "near", "core")


epsilon = 1e-06
masked_score = -1e30
clamp_limit = 7.0
swish_alpha = 1.702


def rms_scaled(values, gain):
    floats = values.astype(jnp.float32)
    return (
        floats
        * lax.rsqrt(jnp.mean(floats * floats, axis=-1, keepdims=True) + epsilon)
        * gain.astype(jnp.float32)
    )


def query_kernel(place_ref, rows_ref, gain_ref, *refs):
    *block_refs, part_ref, own_ref = refs
    count = own_ref.shape[0]
    normed = rms_scaled(rows_ref[...], gain_ref[...]).astype(jnp.bfloat16)
    held = jnp.concatenate([ref[...] for ref in block_refs], axis=0)
    part = lax.dot_general(
        normed, held, (((1,), (1,)), ((), ())), preferred_element_type=jnp.float32
    ).astype(part_ref.dtype)
    own = rows_ref[pl.ds(pl.multiple_of(place_ref[0] * count, count), count)]
    own_ref[...] = rms_scaled(own, gain_ref[...]).astype(own_ref.dtype)
    for i in range(part_ref.shape[0]):
        part_ref[i] = part[i * count : (i + 1) * count]


def query_product(tokens, norm_gain, query_weight):
    count, width = tokens.shape
    members = lax.axis_size(NEAR)
    shard = query_weight.T
    blocks = [shard]
    for d in range(1, members):
        blocks.append(lax.ppermute(shard, NEAR, [(i, i ^ d) for i in range(members)]))
    rows = lax.all_gather(tokens, "far", axis=0, tiled=True)
    far = lax.axis_size("far")
    vmem = pl.BlockSpec(memory_space=pltpu.VMEM)
    smem = pl.BlockSpec(memory_space=pltpu.SMEM)
    return pl.pallas_call(
        query_kernel,
        out_shape=(
            jax.ShapeDtypeStruct((far, count, members * shard.shape[0]), jnp.bfloat16),
            jax.ShapeDtypeStruct((count, width), jnp.bfloat16),
        ),
        in_specs=[smem] + [vmem] * (2 + members),
        out_specs=(vmem, vmem),
        compiler_params=pltpu.CompilerParams(vmem_limit_bytes=24 * 2**20),
        name="query",
    )(
        lax.axis_index("far").astype(jnp.int32).reshape(1),
        rows,
        norm_gain.reshape(1, width),
        *blocks,
    )


def rows_of(ref):
    return jnp.concatenate([ref[i] for i in range(ref.shape[0])], axis=0)


def put_rows(ref, lanes, value):
    per = ref.shape[1]
    for i in range(ref.shape[0]):
        ref[i, :, lanes] = value[i * per : (i + 1) * per]


def attention_kernel(
    group_size, chunk, shard, member_ref, lens_ref, lam_ref, r_ref, nk_ref, nv_ref, gain_ref, disp_ref, k_hbm, v_hbm,
    o_ref, out_ref, k_buf, v_buf, s_buf, q_buf, k_sem, v_sem,
):
    count, heads, width = q_buf.shape
    kv_count = nk_ref.shape[1] // width
    group = heads // kv_count
    half = width // 2
    rows = k_buf.shape[1]
    chunk_rows = chunk * kv_count
    chunks = rows // chunk_rows
    inv_scale = half ** (-0.5)

    def piece(c):
        return pl.ds(pl.multiple_of(c * chunk_rows, chunk_rows), chunk_rows)

    def copies(s, where):
        return (
            pltpu.make_async_copy(k_hbm.at[s, where], k_buf.at[s, where], k_sem.at[s]),
            pltpu.make_async_copy(v_hbm.at[s, where], v_buf.at[s, where], v_sem.at[s]),
        )

    def used(s):
        return (lens_ref[s] + chunk - 1) // chunk

    def fetch(s, _):
        n = used(s)
        for c in range(chunks):
            where = pl.ds(c * chunk_rows, chunk_rows)

            @pl.when(c < n)
            def _():
                for copy in copies(s, where):
                    copy.start()

            @pl.when(c >= n)
            def _():
                v_buf[s, where] = jnp.zeros((chunk_rows, width), v_buf.dtype)

        return 0

    lax.fori_loop(0, count, fetch, 0)

    member = member_ref[0]
    place = lax.broadcasted_iota(jnp.int32, (count, width), 1) // shard
    for h in range(heads):
        head = r_ref[h].astype(jnp.float32)
        bit = 1
        while bit * shard < width:
            turned = jnp.where(
                (place // bit) % 2 == 0,
                pltpu.roll(head, width - bit * shard, 1),
                pltpu.roll(head, bit * shard, 1),
            )
            head = jnp.where((member // bit) % 2 == 1, turned, head)
            bit *= 2
        q_buf[:, h, :] = head

    lane = lax.broadcasted_iota(jnp.int32, (heads, width), 1)
    head_row = lax.broadcasted_iota(jnp.int32, (heads, width), 0)
    column = lax.broadcasted_iota(jnp.int32, (1, heads, rows), 2)
    score_head = lax.broadcasted_iota(jnp.int32, (1, heads, rows), 1)
    own_kv = (column % kv_count) == score_head // group
    position = jnp.where(own_kv, column // kv_count, rows)[None]
    gain = gain_ref[...].astype(jnp.float32)
    lam = jnp.zeros((heads, 1), jnp.float32)
    for h in range(heads):
        lam = jnp.where(head_row[:, :1] == h, lam_ref[h], lam)
    lam = lam[None]
    low = (lane < half)[None]
    block = lax.broadcasted_iota(jnp.int32, (group_size, 1, heads, 1), 0)

    def spread(values):
        out = jnp.zeros((group_size, heads, width), jnp.float32)
        for k in range(kv_count):
            part = values[:, k * width : (k + 1) * width].reshape(group_size, 1, width)
            out = jnp.where((head_row // group == k)[None], part, out)
        return out

    def step(g, _):
        first = g * group_size
        here = pl.ds(first, group_size)
        q = q_buf[here].astype(jnp.bfloat16)
        zero = jnp.zeros_like(q)
        split = jnp.stack([jnp.where(low, q, zero), jnp.where(low, zero, q)], axis=1)
        own_key = spread(nk_ref[here].astype(jnp.float32))
        own_val = spread(nv_ref[here].astype(jnp.float32))
        own_score = (
            jnp.sum(split.astype(jnp.float32) * own_key[:, None], axis=3, keepdims=True) * inv_scale
        )
        limit = jnp.zeros((group_size, 1, heads, 1), jnp.int32)
        for i in range(group_size):
            s = first + i
            limit = jnp.where(block == i, lens_ref[s], limit)

            def wait(c, _):
                for copy in copies(s, piece(c)):
                    copy.wait()
                return 0

            lax.fori_loop(0, used(s), wait, 0)
        for i in range(group_size):
            s_buf[i] = lax.dot_general(
                split[i].reshape(2 * heads, width), k_buf[first + i], (((1,), (1,)), ((), ())), preferred_element_type=jnp.float32
            ).reshape(2, heads, rows)
        scores = jnp.where(position < limit, s_buf[...] * inv_scale, masked_score)
        highest = jnp.maximum(jnp.max(scores, axis=3, keepdims=True), own_score)
        expd = jnp.exp(scores - highest)
        own_exp = jnp.exp(own_score - highest)
        inverse = 1.0 / (jnp.sum(expd, axis=3, keepdims=True) + own_exp)
        plus = inverse[:, 0]
        minus = inverse[:, 1] * lam
        weights = (expd[:, 0] * plus - expd[:, 1] * minus).astype(jnp.bfloat16)
        own_weight = (own_exp[:, 0] * plus - own_exp[:, 1] * minus).astype(jnp.bfloat16)
        attended = jnp.stack(
            [
                jnp.dot(weights[i], v_buf[first + i], preferred_element_type=jnp.float32)
                for i in range(group_size)
            ]
        )
        attended = attended + own_weight.astype(jnp.float32) * own_val
        scale = lax.rsqrt(jnp.mean(attended * attended, axis=2, keepdims=True) + epsilon)
        q_buf[here] = (attended * scale * gain[None]).astype(o_ref.dtype).astype(jnp.float32)
        return 0

    lax.fori_loop(0, count // group_size, step, 0)
    heads_out = jnp.concatenate([q_buf[:, h, :] for h in range(heads)], axis=1).astype(o_ref.dtype)
    o_ref[...] = heads_out
    chosen = disp_ref[...]
    full = jnp.concatenate(
        [heads_out, jnp.zeros((chosen.shape[1] - count, heads * width), o_ref.dtype)], axis=0
    )
    put_rows(
        out_ref,
        pl.ds(0, heads * width),
        jnp.dot(chosen, full, preferred_element_type=jnp.float32).astype(out_ref.dtype),
    )


def attention(
    queries, new_keys, new_values, cache_keys, cache_values, lengths, lambdas, head_gain, dispatch, experts
):
    count, ctx_len, kv_count, width = cache_keys.shape
    heads = lambdas.shape[0]
    slots = dispatch.shape[0]
    shard = heads * width // experts
    vmem = pl.BlockSpec(memory_space=pltpu.VMEM)
    smem = pl.BlockSpec(memory_space=pltpu.SMEM)
    hbm = pl.BlockSpec(memory_space=pltpu.HBM)
    rows = ctx_len * kv_count
    together = 8
    return pl.pallas_call(
        functools.partial(attention_kernel, together, 128, shard),
        out_shape=(
            jax.ShapeDtypeStruct((count, heads * width), jnp.bfloat16),
            jax.ShapeDtypeStruct((experts, slots // experts, heads * width), jnp.bfloat16),
        ),
        in_specs=[smem, smem, smem, vmem, vmem, vmem, vmem, vmem, hbm, hbm],
        out_specs=(vmem, vmem),
        scratch_shapes=[
            pltpu.VMEM((count, rows, width), jnp.bfloat16),
            pltpu.VMEM((count, rows, width), jnp.bfloat16),
            pltpu.VMEM((together, 2, heads, rows), jnp.float32),
            pltpu.VMEM((count, heads, width), jnp.float32),
            pltpu.SemaphoreType.DMA((count,)),
            pltpu.SemaphoreType.DMA((count,)),
        ],
        compiler_params=pltpu.CompilerParams(vmem_limit_bytes=53 * 2**20),
        name="attention",
    )(
        lax.axis_index(NEAR).astype(jnp.int32).reshape(1),
        lengths,
        lambdas,
        queries,
        new_keys,
        new_values,
        head_gain.reshape(1, width),
        dispatch,
        cache_keys.reshape(count, rows, width),
        cache_values.reshape(count, rows, width),
    )


def expert_kernel(
    core_ref, h_ref, rows_ref, own_ref, tok_ref, gain_ref, near_hbm, other_hbm, gate_hbm, up_hbm, down_hbm,
    o_ref, res_ref, wo_buf, gate_buf, up_buf, down_buf, wo_sem, gate_sem, up_sem, down_sem,
):
    core = core_ref[0]
    cols = wo_buf.shape[1] // 2
    depth = wo_buf.shape[2]
    slots = h_ref.shape[0] * h_ref.shape[1]
    pieces = down_sem.shape[0]
    width = o_ref.shape[2]
    step = width // pieces

    wo_copies = []
    for i, source in enumerate((near_hbm, other_hbm)):
        side = core if i == 0 else 1 - core
        at = pl.ds(pl.multiple_of(side * cols, cols), cols)
        wo_copies.append(
            pltpu.make_async_copy(source.at[:, pl.ds(0, cols)], wo_buf.at[:, at], wo_sem.at[i])
        )
    gate_copy = pltpu.make_async_copy(gate_hbm.at[0], gate_buf, gate_sem)
    up_copy = pltpu.make_async_copy(up_hbm.at[0], up_buf, up_sem)
    down_copies = [
        pltpu.make_async_copy(
            down_hbm.at[0, :, pl.ds(i * step, step)], down_buf.at[:, pl.ds(i * step, step)], down_sem.at[i]
        )
        for i in range(pieces)
    ]
    for copy in (*wo_copies, gate_copy, up_copy, *down_copies):
        copy.start()

    heads = jnp.concatenate([rows_of(h_ref), own_ref[...]], axis=0)
    for copy in wo_copies:
        copy.wait()
    attn = lax.dot_general(
        heads,
        wo_buf[...].reshape(width, depth),
        (((1,), (1,)), ((), ())),
        preferred_element_type=jnp.float32,
    ).astype(jnp.bfloat16)
    res_ref[...] = (
        tok_ref[...].astype(jnp.float32) + attn[slots:].astype(jnp.float32)
    ).astype(res_ref.dtype)
    residual = (
        rows_ref[...].astype(jnp.float32) + attn[:slots].astype(jnp.float32)
    ).astype(jnp.bfloat16)
    inputs = rms_scaled(residual, gain_ref[...]).astype(jnp.bfloat16)
    gate_copy.wait()
    gate = jnp.dot(inputs, gate_buf[...], preferred_element_type=jnp.float32)
    gate = jnp.minimum(gate, clamp_limit)
    swish = gate * (1.0 / (1.0 + jnp.exp(-swish_alpha * gate)))
    up_copy.wait()
    upper = jnp.dot(inputs, up_buf[...], preferred_element_type=jnp.float32)
    upper = jnp.clip(upper, -clamp_limit, clamp_limit)
    act = ((upper + 1.0) * swish).astype(jnp.bfloat16)
    for i, copy in enumerate(down_copies):
        copy.wait()
        at = pl.ds(i * step, step)
        put_rows(
            o_ref,
            at,
            jnp.dot(act, down_buf[:, at], preferred_element_type=jnp.float32).astype(o_ref.dtype),
        )


def expert(core, received, rows, head_out, tokens, moe_gain, near, other, cols, gate_w, up_w, down_w):
    members, per, _ = received.shape
    count, width = tokens.shape
    chips, _, depth = near.shape
    hidden = gate_w.shape[2]
    pieces = 4
    vmem = pl.BlockSpec(memory_space=pltpu.VMEM)
    smem = pl.BlockSpec(memory_space=pltpu.SMEM)
    hbm = pl.BlockSpec(memory_space=pltpu.HBM)
    bf16 = jnp.bfloat16
    return pl.pallas_call(
        expert_kernel,
        out_shape=(
            jax.ShapeDtypeStruct((members, per, width), bf16),
            jax.ShapeDtypeStruct((count, width), bf16),
        ),
        in_specs=[smem, vmem, vmem, vmem, vmem, vmem, hbm, hbm, hbm, hbm, hbm],
        out_specs=(vmem, vmem),
        scratch_shapes=[
            pltpu.VMEM((chips, 2 * cols, depth), bf16),
            pltpu.VMEM((width, hidden), bf16),
            pltpu.VMEM((width, hidden), bf16),
            pltpu.VMEM((hidden, width), bf16),
            pltpu.SemaphoreType.DMA((2,)),
            pltpu.SemaphoreType.DMA,
            pltpu.SemaphoreType.DMA,
            pltpu.SemaphoreType.DMA((pieces,)),
        ],
        compiler_params=pltpu.CompilerParams(vmem_limit_bytes=50 * 2**20),
        name="expert",
    )(core, received, rows, head_out, tokens, moe_gain.reshape(1, width), near, other, gate_w, up_w, down_w)


def pick_kernel(cols, count, where_ref, near_hbm, other_hbm, o_ref, x_buf, name_buf, x_sem, name_sem):
    core = where_ref[0]
    expert = where_ref[1].astype(jnp.float32)
    halves, chips, _, depth = x_buf.shape
    names = name_buf.shape[1] // 2
    lanes = name_buf.shape[2]
    members = 2 * chips
    slots = o_ref.shape[0]
    per = slots // members
    copies = []
    for i, source in enumerate((near_hbm, other_hbm)):
        side = core if i == 0 else 1 - core
        at = pl.ds(pl.multiple_of(side * names, names), names)
        first = cols + halves * count
        copies.append(
            pltpu.make_async_copy(
                source.at[:, pl.ds(first, names), pl.ds(0, lanes)], name_buf.at[:, at], name_sem.at[i]
            )
        )
    for i, source in enumerate((near_hbm, other_hbm)):
        side = core if i == 0 else 1 - core
        at = pl.ds(pl.multiple_of(side * count, count), count)
        for half in range(halves):
            rows = pl.ds(cols + half * count, count)
            copies.append(
                pltpu.make_async_copy(
                    source.at[:, rows], x_buf.at[half, :, at], x_sem.at[i * halves + half]
                )
            )
    for copy in copies:
        copy.start()

    def table(shape, rule):
        rows = lax.broadcasted_iota(jnp.int32, shape, 0)
        columns = lax.broadcasted_iota(jnp.int32, shape, 1)
        return jnp.where(rule(rows, columns), 1.0, 0.0).astype(jnp.bfloat16)

    def product(a, b):
        return jnp.dot(a, b, preferred_element_type=jnp.float32)

    for copy in copies[:2]:
        copy.wait()
    named = name_buf[...].reshape(members * names, lanes).astype(jnp.float32)
    found = jnp.where(named == expert, 1.0, 0.0).astype(jnp.bfloat16)
    found = product(table((members, members * names), lambda r, c: c // names == r), found)
    found = found.astype(jnp.bfloat16)
    earlier = product(found, table((lanes, lanes), lambda r, c: r < c)).astype(jnp.bfloat16)
    repeat = table((slots, members), lambda r, c: r // per == c)
    rank = lax.broadcasted_iota(jnp.int32, (slots, lanes), 0) % per
    chosen = jnp.where(
        product(repeat, earlier) == rank.astype(jnp.float32), product(repeat, found), 0.0
    ).astype(jnp.bfloat16)
    spread = product(chosen, table((lanes, members * count), lambda r, c: c % count == r))
    slot = lax.broadcasted_iota(jnp.int32, (slots, members * count), 0)
    column = lax.broadcasted_iota(jnp.int32, (slots, members * count), 1)
    select = jnp.where(slot // per == column // count, spread, 0.0).astype(jnp.bfloat16)
    for copy in copies[2:]:
        copy.wait()
    for half in range(halves):
        o_ref[:, pl.ds(half * depth, depth)] = product(
            select, x_buf[half].reshape(members * count, depth)
        ).astype(o_ref.dtype)


def pick(where, near, other, cols, slots, tokens):
    count, width = tokens.shape
    chips, packed, depth = near.shape
    halves = width // depth
    names = packed - cols - halves * count
    hbm = pl.BlockSpec(memory_space=pltpu.HBM)
    return pl.pallas_call(
        functools.partial(pick_kernel, cols, count),
        out_shape=jax.ShapeDtypeStruct((slots, width), jnp.bfloat16),
        in_specs=[pl.BlockSpec(memory_space=pltpu.SMEM), hbm, hbm],
        out_specs=pl.BlockSpec(memory_space=pltpu.VMEM),
        scratch_shapes=[
            pltpu.VMEM((halves, chips, 2 * count, depth), jnp.bfloat16),
            pltpu.VMEM((chips, 2 * names, 128), jnp.bfloat16),
            pltpu.SemaphoreType.DMA((2 * halves,)),
            pltpu.SemaphoreType.DMA((2,)),
        ],
        compiler_params=pltpu.CompilerParams(vmem_limit_bytes=50 * 2**20),
        name="pick",
    )(where, near, other)


def combine_kernel(share_ref, rows_ref, res_ref, o_ref):
    share = share_ref[...]
    high = share.astype(jnp.bfloat16)
    low = (share - high.astype(jnp.float32)).astype(jnp.bfloat16)
    rows = rows_of(rows_ref)
    total = jnp.dot(high, rows, preferred_element_type=jnp.float32) + jnp.dot(
        low, rows, preferred_element_type=jnp.float32
    )
    o_ref[...] = (res_ref[...].astype(jnp.float32) + total).astype(o_ref.dtype)


def combine(share, rows, residual):
    vmem = pl.BlockSpec(memory_space=pltpu.VMEM)
    return pl.pallas_call(
        combine_kernel,
        out_shape=jax.ShapeDtypeStruct(residual.shape, jnp.bfloat16),
        in_specs=[vmem] * 3,
        out_specs=vmem,
        compiler_params=pltpu.CompilerParams(vmem_limit_bytes=32 * 2**20),
        name="combine",
    )(share, rows, residual)


def local(
    tokens,
    norm_gain,
    query_weight,
    key_weight,
    value_weight,
    out_weight,
    head_gain,
    lambdas,
    cache_keys,
    cache_values,
    lengths,
    moe_gain,
    gate_weight,
    up_weight,
    down_weight,
    routes,
    route_weights,
):
    count = tokens.shape[0]
    topk = routes.shape[1]
    depth = out_weight.shape[0]
    named = jnp.pad(
        routes.T.astype(jnp.bfloat16), ((0, 8 - topk), (0, depth - count)), constant_values=-1
    )
    packed = jnp.concatenate([out_weight.T, tokens[:, :depth], tokens[:, depth:], named], axis=0)
    near_packed = lax.all_gather(packed, CHIPS, axis=0)
    part, normed = query_product(tokens, norm_gain, query_weight)
    queries = lax.all_to_all(part, "far", 0, 0, tiled=True)
    new_keys = jnp.dot(normed, key_weight, preferred_element_type=jnp.float32).astype(jnp.bfloat16)
    new_values = jnp.dot(normed, value_weight, preferred_element_type=jnp.float32).astype(
        jnp.bfloat16
    )
    experts = lax.axis_size(EP)
    capacity = min(count, max(2, 2 * count * topk // experts))
    routes, new_keys = lax.optimization_barrier((routes, new_keys))
    slot_range = jnp.arange(experts * capacity, dtype=jnp.int32)
    onehot = (
        routes.reshape(-1)[:, None] == jnp.arange(experts, dtype=jnp.int32)[None, :]
    ).astype(jnp.int32)
    earlier_all = jnp.cumsum(onehot, axis=0) - onehot
    ranks = jnp.sum(earlier_all * onehot, axis=1).reshape(count, topk)
    slot_id = routes * capacity + ranks
    dispatch = jnp.any(slot_id[None, :, :] == slot_range[:, None, None], axis=2).astype(
        jnp.bfloat16
    )
    dispatch = jnp.pad(dispatch, ((0, 0), (0, 128 - count)))
    share = jnp.sum(
        jnp.where(slot_id[:, :, None] == slot_range[None, None, :], route_weights[:, :, None], 0.0),
        axis=1,
    )
    head_out, outgoing = attention(
        queries, new_keys, new_values, cache_keys, cache_values, lengths, lambdas, head_gain, dispatch, experts
    )
    received = lax.all_to_all(outgoing, EP, split_axis=0, concat_axis=0, tiled=True)
    near_packed, head_out = lax.optimization_barrier((near_packed, head_out))
    other_packed = lax.ppermute(near_packed, "core", [(0, 1), (1, 0)])
    core = lax.axis_index("core").astype(jnp.int32)
    where = jnp.stack([core, lax.axis_index(EP).astype(jnp.int32)])
    cols = out_weight.shape[1]
    rows = pick(where, near_packed, other_packed, cols, experts * capacity, tokens)
    results, residual = expert(
        where,
        received,
        rows,
        head_out,
        tokens,
        moe_gain,
        near_packed,
        other_packed,
        cols,
        gate_weight,
        up_weight,
        down_weight,
    )
    returned = lax.all_to_all(results, EP, split_axis=0, concat_axis=0, tiled=True)
    return combine(share, returned, residual)


def solution(mesh):
    devices = mesh.devices.reshape(mesh.shape["grp"], -1, 2, 2)
    torus = Mesh(devices, ("grp", "far", "near", "core"))
    return jax.shard_map(
        local,
        mesh=torus,
        in_specs=(
            P(GRP_EP, None),
            P(),
            P(None, EP),
            P(),
            P(),
            P(None, EP),
            P(),
            P(),
            P(GRP_EP, None, None, None),
            P(GRP_EP, None, None, None),
            P(GRP_EP),
            P(),
            P(EP, None, None),
            P(EP, None, None),
            P(EP, None, None),
            P(GRP_EP, None),
            P(GRP_EP, None),
        ),
        out_specs=P(GRP_EP, None),
        check_vma=False,
    )
```

```python
import functools

import jax
import jax.numpy as jnp
from jax import lax
from jax.experimental import pallas as pl
from jax.experimental.pallas import tpu as pltpu
from jax.sharding import Mesh
from jax.sharding import PartitionSpec as P


EP = ("far", "near", "core")
NEAR = ("near", "core")
CHIPS = ("far", "near")
GRP_EP = ("grp", "far", "near", "core")


epsilon = 1e-06
masked_score = -1e30
clamp_limit = 7.0
swish_alpha = 1.702


def rms_scaled(values, gain):
    floats = values.astype(jnp.float32)
    return (
        floats
        * lax.rsqrt(jnp.mean(floats * floats, axis=-1, keepdims=True) + epsilon)
        * gain.astype(jnp.float32)
    )


def pack_kernel(weight_hbm, tokens_hbm, routes_ref, o_hbm, name_buf, sem):
    cols, depth = weight_hbm.shape
    count, width = tokens_hbm.shape
    copies = [pltpu.make_async_copy(weight_hbm, o_hbm.at[pl.ds(0, cols)], sem.at[0])]
    for half in range(width // depth):
        copies.append(
            pltpu.make_async_copy(
                tokens_hbm.at[:, pl.ds(half * depth, depth)],
                o_hbm.at[pl.ds(cols + half * count, count)],
                sem.at[1 + half],
            )
        )
    for copy in copies:
        copy.start()
    named = routes_ref[...].astype(jnp.float32)
    named = jnp.concatenate([named, jnp.full((name_buf.shape[0] - named.shape[0], count), -1.0)], axis=0)
    rest = jnp.full((name_buf.shape[0], depth - count), -1.0, jnp.float32)
    name_buf[...] = jnp.concatenate([named, rest], axis=1).astype(name_buf.dtype)
    first = o_hbm.shape[0] - name_buf.shape[0]
    copies.append(
        pltpu.make_async_copy(name_buf, o_hbm.at[pl.ds(first, name_buf.shape[0])], sem.at[len(copies)])
    )
    copies[-1].start()
    for copy in copies:
        copy.wait()


def pack(out_weight, tokens, routes):
    depth, cols = out_weight.shape
    count, width = tokens.shape
    halves = width // depth
    hbm = pl.BlockSpec(memory_space=pltpu.HBM)
    return pl.pallas_call(
        pack_kernel,
        out_shape=jax.ShapeDtypeStruct((cols + halves * count + 8, depth), jnp.bfloat16),
        in_specs=[hbm, hbm, pl.BlockSpec(memory_space=pltpu.VMEM)],
        out_specs=hbm,
        scratch_shapes=[pltpu.VMEM((8, depth), jnp.bfloat16), pltpu.SemaphoreType.DMA((2 + halves,))],
        name="pack",
    )(out_weight.T, tokens, routes.T)


def query_kernel(place_ref, rows_ref, gain_ref, *refs):
    *block_refs, part_ref, own_ref = refs
    count = own_ref.shape[0]
    normed = rms_scaled(rows_ref[...], gain_ref[...]).astype(jnp.bfloat16)
    held = jnp.concatenate([ref[...] for ref in block_refs], axis=0)
    part = lax.dot_general(
        normed, held, (((1,), (1,)), ((), ())), preferred_element_type=jnp.float32
    ).astype(part_ref.dtype)
    own = rows_ref[pl.ds(pl.multiple_of(place_ref[0] * count, count), count)]
    own_ref[...] = rms_scaled(own, gain_ref[...]).astype(own_ref.dtype)
    for i in range(part_ref.shape[0]):
        part_ref[i] = part[i * count : (i + 1) * count]


def query_product(tokens, norm_gain, query_weight):
    count, width = tokens.shape
    members = lax.axis_size(NEAR)
    shard = query_weight.T
    blocks = [shard]
    for d in range(1, members):
        blocks.append(lax.ppermute(shard, NEAR, [(i, i ^ d) for i in range(members)]))
    rows = lax.all_gather(tokens, "far", axis=0, tiled=True)
    far = lax.axis_size("far")
    vmem = pl.BlockSpec(memory_space=pltpu.VMEM)
    smem = pl.BlockSpec(memory_space=pltpu.SMEM)
    return pl.pallas_call(
        query_kernel,
        out_shape=(
            jax.ShapeDtypeStruct((far, count, members * shard.shape[0]), jnp.bfloat16),
            jax.ShapeDtypeStruct((count, width), jnp.bfloat16),
        ),
        in_specs=[smem] + [vmem] * (2 + members),
        out_specs=(vmem, vmem),
        compiler_params=pltpu.CompilerParams(vmem_limit_bytes=24 * 2**20),
        name="query",
    )(
        lax.axis_index("far").astype(jnp.int32).reshape(1),
        rows,
        norm_gain.reshape(1, width),
        *blocks,
    )


def rows_of(ref):
    return jnp.concatenate([ref[i] for i in range(ref.shape[0])], axis=0)


def put_rows(ref, lanes, value):
    per = ref.shape[1]
    for i in range(ref.shape[0]):
        ref[i, :, lanes] = value[i * per : (i + 1) * per]


def attention_kernel(
    group_size, chunk, shard, member_ref, lens_ref, lam_ref, r_ref, nk_ref, nv_ref, gain_ref, disp_ref, k_hbm, v_hbm,
    o_ref, out_ref, k_buf, v_buf, s_buf, q_buf, k_sem, v_sem,
):
    count, heads, width = q_buf.shape
    kv_count = nk_ref.shape[1] // width
    group = heads // kv_count
    half = width // 2
    rows = k_buf.shape[1]
    chunk_rows = chunk * kv_count
    chunks = rows // chunk_rows
    inv_scale = half ** (-0.5)

    def piece(c):
        return pl.ds(pl.multiple_of(c * chunk_rows, chunk_rows), chunk_rows)

    def copies(s, where):
        return (
            pltpu.make_async_copy(k_hbm.at[s, where], k_buf.at[s, where], k_sem.at[s]),
            pltpu.make_async_copy(v_hbm.at[s, where], v_buf.at[s, where], v_sem.at[s]),
        )

    def used(s):
        return (lens_ref[s] + chunk - 1) // chunk

    def fetch(s, _):
        n = used(s)
        for c in range(chunks):
            where = pl.ds(c * chunk_rows, chunk_rows)

            @pl.when(c < n)
            def _():
                for copy in copies(s, where):
                    copy.start()

            @pl.when(c >= n)
            def _():
                v_buf[s, where] = jnp.zeros((chunk_rows, width), v_buf.dtype)

        return 0

    lax.fori_loop(0, count, fetch, 0)

    member = member_ref[0]
    place = lax.broadcasted_iota(jnp.int32, (count, width), 1) // shard
    for h in range(heads):
        head = r_ref[h].astype(jnp.float32)
        bit = 1
        while bit * shard < width:
            turned = jnp.where(
                (place // bit) % 2 == 0,
                pltpu.roll(head, width - bit * shard, 1),
                pltpu.roll(head, bit * shard, 1),
            )
            head = jnp.where((member // bit) % 2 == 1, turned, head)
            bit *= 2
        q_buf[:, h, :] = head

    lane = lax.broadcasted_iota(jnp.int32, (heads, width), 1)
    head_row = lax.broadcasted_iota(jnp.int32, (heads, width), 0)
    column = lax.broadcasted_iota(jnp.int32, (1, heads, rows), 2)
    score_head = lax.broadcasted_iota(jnp.int32, (1, heads, rows), 1)
    own_kv = (column % kv_count) == score_head // group
    position = jnp.where(own_kv, column // kv_count, rows)[None]
    gain = gain_ref[...].astype(jnp.float32)
    lam = jnp.zeros((heads, 1), jnp.float32)
    for h in range(heads):
        lam = jnp.where(head_row[:, :1] == h, lam_ref[h], lam)
    lam = lam[None]
    low = (lane < half)[None]
    block = lax.broadcasted_iota(jnp.int32, (group_size, 1, heads, 1), 0)

    def spread(values):
        out = jnp.zeros((group_size, heads, width), jnp.float32)
        for k in range(kv_count):
            part = values[:, k * width : (k + 1) * width].reshape(group_size, 1, width)
            out = jnp.where((head_row // group == k)[None], part, out)
        return out

    def step(g, _):
        first = g * group_size
        here = pl.ds(first, group_size)
        q = q_buf[here].astype(jnp.bfloat16)
        zero = jnp.zeros_like(q)
        split = jnp.stack([jnp.where(low, q, zero), jnp.where(low, zero, q)], axis=1)
        own_key = spread(nk_ref[here].astype(jnp.float32))
        own_val = spread(nv_ref[here].astype(jnp.float32))
        own_score = (
            jnp.sum(split.astype(jnp.float32) * own_key[:, None], axis=3, keepdims=True) * inv_scale
        )
        limit = jnp.zeros((group_size, 1, heads, 1), jnp.int32)
        for i in range(group_size):
            s = first + i
            limit = jnp.where(block == i, lens_ref[s], limit)

            def wait(c, _):
                for copy in copies(s, piece(c)):
                    copy.wait()
                return 0

            lax.fori_loop(0, used(s), wait, 0)
        for i in range(group_size):
            s_buf[i] = lax.dot_general(
                split[i].reshape(2 * heads, width), k_buf[first + i], (((1,), (1,)), ((), ())), preferred_element_type=jnp.float32
            ).reshape(2, heads, rows)
        scores = jnp.where(position < limit, s_buf[...] * inv_scale, masked_score)
        highest = jnp.maximum(jnp.max(scores, axis=3, keepdims=True), own_score)
        expd = jnp.exp(scores - highest)
        own_exp = jnp.exp(own_score - highest)
        inverse = 1.0 / (jnp.sum(expd, axis=3, keepdims=True) + own_exp)
        plus = inverse[:, 0]
        minus = inverse[:, 1] * lam
        weights = (expd[:, 0] * plus - expd[:, 1] * minus).astype(jnp.bfloat16)
        own_weight = (own_exp[:, 0] * plus - own_exp[:, 1] * minus).astype(jnp.bfloat16)
        attended = jnp.stack(
            [
                jnp.dot(weights[i], v_buf[first + i], preferred_element_type=jnp.float32)
                for i in range(group_size)
            ]
        )
        attended = attended + own_weight.astype(jnp.float32) * own_val
        scale = lax.rsqrt(jnp.mean(attended * attended, axis=2, keepdims=True) + epsilon)
        q_buf[here] = (attended * scale * gain[None]).astype(o_ref.dtype).astype(jnp.float32)
        return 0

    lax.fori_loop(0, count // group_size, step, 0)
    heads_out = jnp.concatenate([q_buf[:, h, :] for h in range(heads)], axis=1).astype(o_ref.dtype)
    o_ref[...] = heads_out
    chosen = disp_ref[...]
    full = jnp.concatenate(
        [heads_out, jnp.zeros((chosen.shape[1] - count, heads * width), o_ref.dtype)], axis=0
    )
    put_rows(
        out_ref,
        pl.ds(0, heads * width),
        jnp.dot(chosen, full, preferred_element_type=jnp.float32).astype(out_ref.dtype),
    )


def attention(
    queries, new_keys, new_values, cache_keys, cache_values, lengths, lambdas, head_gain, dispatch, experts
):
    count, ctx_len, kv_count, width = cache_keys.shape
    heads = lambdas.shape[0]
    slots = dispatch.shape[0]
    shard = heads * width // experts
    vmem = pl.BlockSpec(memory_space=pltpu.VMEM)
    smem = pl.BlockSpec(memory_space=pltpu.SMEM)
    hbm = pl.BlockSpec(memory_space=pltpu.HBM)
    rows = ctx_len * kv_count
    together = 8
    return pl.pallas_call(
        functools.partial(attention_kernel, together, 128, shard),
        out_shape=(
            jax.ShapeDtypeStruct((count, heads * width), jnp.bfloat16),
            jax.ShapeDtypeStruct((experts, slots // experts, heads * width), jnp.bfloat16),
        ),
        in_specs=[smem, smem, smem, vmem, vmem, vmem, vmem, vmem, hbm, hbm],
        out_specs=(vmem, vmem),
        scratch_shapes=[
            pltpu.VMEM((count, rows, width), jnp.bfloat16),
            pltpu.VMEM((count, rows, width), jnp.bfloat16),
            pltpu.VMEM((together, 2, heads, rows), jnp.float32),
            pltpu.VMEM((count, heads, width), jnp.float32),
            pltpu.SemaphoreType.DMA((count,)),
            pltpu.SemaphoreType.DMA((count,)),
        ],
        compiler_params=pltpu.CompilerParams(vmem_limit_bytes=53 * 2**20),
        name="attention",
    )(
        lax.axis_index(NEAR).astype(jnp.int32).reshape(1),
        lengths,
        lambdas,
        queries,
        new_keys,
        new_values,
        head_gain.reshape(1, width),
        dispatch,
        cache_keys.reshape(count, rows, width),
        cache_values.reshape(count, rows, width),
    )


def expert_kernel(
    core_ref, h_ref, rows_ref, own_ref, tok_ref, gain_ref, near_hbm, other_hbm, gate_hbm, up_hbm, down_hbm,
    o_ref, res_ref, wo_buf, gate_buf, up_buf, down_buf, wo_sem, gate_sem, up_sem, down_sem,
):
    core = core_ref[0]
    cols = wo_buf.shape[1] // 2
    depth = wo_buf.shape[2]
    slots = h_ref.shape[0] * h_ref.shape[1]
    pieces = down_sem.shape[0]
    width = o_ref.shape[2]
    step = width // pieces

    wo_copies = []
    for i, source in enumerate((near_hbm, other_hbm)):
        side = core if i == 0 else 1 - core
        at = pl.ds(pl.multiple_of(side * cols, cols), cols)
        wo_copies.append(
            pltpu.make_async_copy(source.at[:, pl.ds(0, cols)], wo_buf.at[:, at], wo_sem.at[i])
        )
    gate_copy = pltpu.make_async_copy(gate_hbm.at[0], gate_buf, gate_sem)
    up_copy = pltpu.make_async_copy(up_hbm.at[0], up_buf, up_sem)
    down_copies = [
        pltpu.make_async_copy(
            down_hbm.at[0, :, pl.ds(i * step, step)], down_buf.at[:, pl.ds(i * step, step)], down_sem.at[i]
        )
        for i in range(pieces)
    ]
    for copy in (*wo_copies, gate_copy, up_copy, *down_copies):
        copy.start()

    heads = jnp.concatenate([rows_of(h_ref), own_ref[...]], axis=0)
    for copy in wo_copies:
        copy.wait()
    attn = lax.dot_general(
        heads,
        wo_buf[...].reshape(width, depth),
        (((1,), (1,)), ((), ())),
        preferred_element_type=jnp.float32,
    ).astype(jnp.bfloat16)
    res_ref[...] = (
        tok_ref[...].astype(jnp.float32) + attn[slots:].astype(jnp.float32)
    ).astype(res_ref.dtype)
    residual = (
        rows_ref[...].astype(jnp.float32) + attn[:slots].astype(jnp.float32)
    ).astype(jnp.bfloat16)
    inputs = rms_scaled(residual, gain_ref[...]).astype(jnp.bfloat16)
    gate_copy.wait()
    gate = jnp.dot(inputs, gate_buf[...], preferred_element_type=jnp.float32)
    gate = jnp.minimum(gate, clamp_limit)
    swish = gate * (1.0 / (1.0 + jnp.exp(-swish_alpha * gate)))
    up_copy.wait()
    upper = jnp.dot(inputs, up_buf[...], preferred_element_type=jnp.float32)
    upper = jnp.clip(upper, -clamp_limit, clamp_limit)
    act = ((upper + 1.0) * swish).astype(jnp.bfloat16)
    for i, copy in enumerate(down_copies):
        copy.wait()
        at = pl.ds(i * step, step)
        put_rows(
            o_ref,
            at,
            jnp.dot(act, down_buf[:, at], preferred_element_type=jnp.float32).astype(o_ref.dtype),
        )


def expert(core, received, rows, head_out, tokens, moe_gain, near, other, cols, gate_w, up_w, down_w):
    members, per, _ = received.shape
    count, width = tokens.shape
    chips, _, depth = near.shape
    hidden = gate_w.shape[2]
    pieces = 4
    vmem = pl.BlockSpec(memory_space=pltpu.VMEM)
    smem = pl.BlockSpec(memory_space=pltpu.SMEM)
    hbm = pl.BlockSpec(memory_space=pltpu.HBM)
    bf16 = jnp.bfloat16
    return pl.pallas_call(
        expert_kernel,
        out_shape=(
            jax.ShapeDtypeStruct((members, per, width), bf16),
            jax.ShapeDtypeStruct((count, width), bf16),
        ),
        in_specs=[smem, vmem, vmem, vmem, vmem, vmem, hbm, hbm, hbm, hbm, hbm],
        out_specs=(vmem, vmem),
        scratch_shapes=[
            pltpu.VMEM((chips, 2 * cols, depth), bf16),
            pltpu.VMEM((width, hidden), bf16),
            pltpu.VMEM((width, hidden), bf16),
            pltpu.VMEM((hidden, width), bf16),
            pltpu.SemaphoreType.DMA((2,)),
            pltpu.SemaphoreType.DMA,
            pltpu.SemaphoreType.DMA,
            pltpu.SemaphoreType.DMA((pieces,)),
        ],
        compiler_params=pltpu.CompilerParams(vmem_limit_bytes=50 * 2**20),
        name="expert",
    )(core, received, rows, head_out, tokens, moe_gain.reshape(1, width), near, other, gate_w, up_w, down_w)


def pick_kernel(cols, count, where_ref, near_hbm, other_hbm, o_ref, x_buf, name_buf, x_sem, name_sem):
    core = where_ref[0]
    expert = where_ref[1].astype(jnp.float32)
    halves, chips, _, depth = x_buf.shape
    names = name_buf.shape[1] // 2
    lanes = name_buf.shape[2]
    members = 2 * chips
    slots = o_ref.shape[0]
    per = slots // members
    copies = []
    for i, source in enumerate((near_hbm, other_hbm)):
        side = core if i == 0 else 1 - core
        at = pl.ds(pl.multiple_of(side * names, names), names)
        first = cols + halves * count
        copies.append(
            pltpu.make_async_copy(
                source.at[:, pl.ds(first, names), pl.ds(0, lanes)], name_buf.at[:, at], name_sem.at[i]
            )
        )
    for i, source in enumerate((near_hbm, other_hbm)):
        side = core if i == 0 else 1 - core
        at = pl.ds(pl.multiple_of(side * count, count), count)
        for half in range(halves):
            rows = pl.ds(cols + half * count, count)
            copies.append(
                pltpu.make_async_copy(
                    source.at[:, rows], x_buf.at[half, :, at], x_sem.at[i * halves + half]
                )
            )
    for copy in copies:
        copy.start()

    def table(shape, rule):
        rows = lax.broadcasted_iota(jnp.int32, shape, 0)
        columns = lax.broadcasted_iota(jnp.int32, shape, 1)
        return jnp.where(rule(rows, columns), 1.0, 0.0).astype(jnp.bfloat16)

    def product(a, b):
        return jnp.dot(a, b, preferred_element_type=jnp.float32)

    for copy in copies[:2]:
        copy.wait()
    named = name_buf[...].reshape(members * names, lanes).astype(jnp.float32)
    found = jnp.where(named == expert, 1.0, 0.0).astype(jnp.bfloat16)
    found = product(table((members, members * names), lambda r, c: c // names == r), found)
    found = found.astype(jnp.bfloat16)
    earlier = product(found, table((lanes, lanes), lambda r, c: r < c)).astype(jnp.bfloat16)
    repeat = table((slots, members), lambda r, c: r // per == c)
    rank = lax.broadcasted_iota(jnp.int32, (slots, lanes), 0) % per
    chosen = jnp.where(
        product(repeat, earlier) == rank.astype(jnp.float32), product(repeat, found), 0.0
    ).astype(jnp.bfloat16)
    spread = product(chosen, table((lanes, members * count), lambda r, c: c % count == r))
    slot = lax.broadcasted_iota(jnp.int32, (slots, members * count), 0)
    column = lax.broadcasted_iota(jnp.int32, (slots, members * count), 1)
    select = jnp.where(slot // per == column // count, spread, 0.0).astype(jnp.bfloat16)
    for copy in copies[2:]:
        copy.wait()
    for half in range(halves):
        o_ref[:, pl.ds(half * depth, depth)] = product(
            select, x_buf[half].reshape(members * count, depth)
        ).astype(o_ref.dtype)


def pick(where, near, other, cols, slots, tokens):
    count, width = tokens.shape
    chips, packed, depth = near.shape
    halves = width // depth
    names = packed - cols - halves * count
    hbm = pl.BlockSpec(memory_space=pltpu.HBM)
    return pl.pallas_call(
        functools.partial(pick_kernel, cols, count),
        out_shape=jax.ShapeDtypeStruct((slots, width), jnp.bfloat16),
        in_specs=[pl.BlockSpec(memory_space=pltpu.SMEM), hbm, hbm],
        out_specs=pl.BlockSpec(memory_space=pltpu.VMEM),
        scratch_shapes=[
            pltpu.VMEM((halves, chips, 2 * count, depth), jnp.bfloat16),
            pltpu.VMEM((chips, 2 * names, 128), jnp.bfloat16),
            pltpu.SemaphoreType.DMA((2 * halves,)),
            pltpu.SemaphoreType.DMA((2,)),
        ],
        compiler_params=pltpu.CompilerParams(vmem_limit_bytes=50 * 2**20),
        name="pick",
    )(where, near, other)


def combine_kernel(share_ref, rows_ref, res_ref, o_ref):
    share = share_ref[...]
    high = share.astype(jnp.bfloat16)
    low = (share - high.astype(jnp.float32)).astype(jnp.bfloat16)
    rows = rows_of(rows_ref)
    total = jnp.dot(high, rows, preferred_element_type=jnp.float32) + jnp.dot(
        low, rows, preferred_element_type=jnp.float32
    )
    o_ref[...] = (res_ref[...].astype(jnp.float32) + total).astype(o_ref.dtype)


def combine(share, rows, residual):
    vmem = pl.BlockSpec(memory_space=pltpu.VMEM)
    return pl.pallas_call(
        combine_kernel,
        out_shape=jax.ShapeDtypeStruct(residual.shape, jnp.bfloat16),
        in_specs=[vmem] * 3,
        out_specs=vmem,
        compiler_params=pltpu.CompilerParams(vmem_limit_bytes=32 * 2**20),
        name="combine",
    )(share, rows, residual)


def local(
    tokens,
    norm_gain,
    query_weight,
    key_weight,
    value_weight,
    out_weight,
    head_gain,
    lambdas,
    cache_keys,
    cache_values,
    lengths,
    moe_gain,
    gate_weight,
    up_weight,
    down_weight,
    routes,
    route_weights,
):
    count = tokens.shape[0]
    topk = routes.shape[1]
    packed = pack(out_weight, tokens, routes)
    near_packed = lax.all_gather(packed, CHIPS, axis=0)
    part, normed = query_product(tokens, norm_gain, query_weight)
    queries = lax.all_to_all(part, "far", 0, 0, tiled=True)
    new_keys = jnp.dot(normed, key_weight, preferred_element_type=jnp.float32).astype(
        jnp.bfloat16
    )
    new_values = jnp.dot(normed, value_weight, preferred_element_type=jnp.float32).astype(
        jnp.bfloat16
    )
    experts = lax.axis_size(EP)
    capacity = min(count, max(2, 2 * count * topk // experts))
    routes, new_keys = lax.optimization_barrier((routes, new_keys))
    slot_range = jnp.arange(experts * capacity, dtype=jnp.int32)
    onehot = (
        routes.reshape(-1)[:, None] == jnp.arange(experts, dtype=jnp.int32)[None, :]
    ).astype(jnp.int32)
    earlier_all = jnp.cumsum(onehot, axis=0) - onehot
    ranks = jnp.sum(earlier_all * onehot, axis=1).reshape(count, topk)
    slot_id = routes * capacity + ranks
    dispatch = jnp.any(slot_id[None, :, :] == slot_range[:, None, None], axis=2).astype(
        jnp.bfloat16
    )
    dispatch = jnp.pad(dispatch, ((0, 0), (0, 128 - count)))
    share = jnp.sum(
        jnp.where(slot_id[:, :, None] == slot_range[None, None, :], route_weights[:, :, None], 0.0),
        axis=1,
    )
    head_out, outgoing = attention(
        queries, new_keys, new_values, cache_keys, cache_values, lengths, lambdas, head_gain, dispatch, experts
    )
    received = lax.all_to_all(outgoing, EP, split_axis=0, concat_axis=0, tiled=True)
    near_packed, head_out = lax.optimization_barrier((near_packed, head_out))
    other_packed = lax.ppermute(near_packed, "core", [(0, 1), (1, 0)])
    core = lax.axis_index("core").astype(jnp.int32)
    where = jnp.stack([core, lax.axis_index(EP).astype(jnp.int32)])
    cols = out_weight.shape[1]
    rows = pick(where, near_packed, other_packed, cols, experts * capacity, tokens)
    results, residual = expert(
        where,
        received,
        rows,
        head_out,
        tokens,
        moe_gain,
        near_packed,
        other_packed,
        cols,
        gate_weight,
        up_weight,
        down_weight,
    )
    returned = lax.all_to_all(results, EP, split_axis=0, concat_axis=0, tiled=True)
    return combine(share, returned, residual)


def solution(mesh):
    devices = mesh.devices.reshape(mesh.shape["grp"], -1, 2, 2)
    torus = Mesh(devices, ("grp", "far", "near", "core"))
    return jax.shard_map(
        local,
        mesh=torus,
        in_specs=(
            P(GRP_EP, None),
            P(),
            P(None, EP),
            P(),
            P(),
            P(None, EP),
            P(),
            P(),
            P(GRP_EP, None, None, None),
            P(GRP_EP, None, None, None),
            P(GRP_EP),
            P(),
            P(EP, None, None),
            P(EP, None, None),
            P(EP, None, None),
            P(GRP_EP, None),
            P(GRP_EP, None),
        ),
        out_specs=P(GRP_EP, None),
        check_vma=False,
    )
```

```python
import functools

import jax
import jax.numpy as jnp
from jax import lax
from jax.experimental import pallas as pl
from jax.experimental.pallas import tpu as pltpu
from jax.sharding import Mesh
from jax.sharding import PartitionSpec as P


EP = ("far", "near", "core")
NEAR = ("near", "core")
CHIPS = ("far", "near")
GRP_EP = ("grp", "far", "near", "core")


epsilon = 1e-06
masked_score = -1e30
clamp_limit = 7.0
swish_alpha = 1.702


def rms_scaled(values, gain):
    floats = values.astype(jnp.float32)
    return (
        floats
        * lax.rsqrt(jnp.mean(floats * floats, axis=-1, keepdims=True) + epsilon)
        * gain.astype(jnp.float32)
    )


def pack_kernel(weight_ref, tokens_ref, routes_ref, o_ref):
    cols, depth = weight_ref.shape
    count, width = tokens_ref.shape
    halves = width // depth
    o_ref[pl.ds(0, cols)] = weight_ref[...]
    for half in range(halves):
        o_ref[pl.ds(cols + half * count, count)] = tokens_ref[:, pl.ds(half * depth, depth)]
    first = cols + halves * count
    named = routes_ref[...].astype(jnp.float32)
    rows = o_ref.shape[0] - first
    named = jnp.concatenate([named, jnp.full((rows - named.shape[0], count), -1.0)], axis=0)
    rest = jnp.full((rows, depth - count), -1.0, jnp.float32)
    o_ref[pl.ds(first, rows)] = jnp.concatenate([named, rest], axis=1).astype(o_ref.dtype)


def pack(out_weight, tokens, routes):
    depth, cols = out_weight.shape
    count, width = tokens.shape
    vmem = pl.BlockSpec(memory_space=pltpu.VMEM)
    return pl.pallas_call(
        pack_kernel,
        out_shape=jax.ShapeDtypeStruct((cols + width // depth * count + 8, depth), jnp.bfloat16),
        in_specs=[vmem] * 3,
        out_specs=vmem,
        name="pack",
    )(out_weight.T, tokens, routes.T)


def query_kernel(place_ref, rows_ref, gain_ref, *refs):
    *block_refs, part_ref, own_ref = refs
    count = own_ref.shape[0]
    normed = rms_scaled(rows_ref[...], gain_ref[...]).astype(jnp.bfloat16)
    held = jnp.concatenate([ref[...] for ref in block_refs], axis=0)
    part = lax.dot_general(
        normed, held, (((1,), (1,)), ((), ())), preferred_element_type=jnp.float32
    ).astype(part_ref.dtype)
    own = rows_ref[pl.ds(pl.multiple_of(place_ref[0] * count, count), count)]
    own_ref[...] = rms_scaled(own, gain_ref[...]).astype(own_ref.dtype)
    for i in range(part_ref.shape[0]):
        part_ref[i] = part[i * count : (i + 1) * count]


def query_product(tokens, norm_gain, query_weight):
    count, width = tokens.shape
    members = lax.axis_size(NEAR)
    shard = query_weight.T
    blocks = [shard]
    for d in range(1, members):
        blocks.append(lax.ppermute(shard, NEAR, [(i, i ^ d) for i in range(members)]))
    rows = lax.all_gather(tokens, "far", axis=0, tiled=True)
    far = lax.axis_size("far")
    vmem = pl.BlockSpec(memory_space=pltpu.VMEM)
    smem = pl.BlockSpec(memory_space=pltpu.SMEM)
    return pl.pallas_call(
        query_kernel,
        out_shape=(
            jax.ShapeDtypeStruct((far, count, members * shard.shape[0]), jnp.bfloat16),
            jax.ShapeDtypeStruct((count, width), jnp.bfloat16),
        ),
        in_specs=[smem] + [vmem] * (2 + members),
        out_specs=(vmem, vmem),
        compiler_params=pltpu.CompilerParams(vmem_limit_bytes=24 * 2**20),
        name="query",
    )(
        lax.axis_index("far").astype(jnp.int32).reshape(1),
        rows,
        norm_gain.reshape(1, width),
        *blocks,
    )


def rows_of(ref):
    return jnp.concatenate([ref[i] for i in range(ref.shape[0])], axis=0)


def put_rows(ref, lanes, value):
    per = ref.shape[1]
    for i in range(ref.shape[0]):
        ref[i, :, lanes] = value[i * per : (i + 1) * per]


def attention_kernel(
    group_size, chunk, shard, member_ref, lens_ref, lam_ref, r_ref, nk_ref, nv_ref, gain_ref, disp_ref, k_hbm, v_hbm,
    o_ref, out_ref, k_buf, v_buf, s_buf, q_buf, k_sem, v_sem,
):
    count, heads, width = q_buf.shape
    kv_count = nk_ref.shape[1] // width
    group = heads // kv_count
    half = width // 2
    rows = k_buf.shape[1]
    chunk_rows = chunk * kv_count
    chunks = rows // chunk_rows
    inv_scale = half ** (-0.5)

    def piece(c):
        return pl.ds(pl.multiple_of(c * chunk_rows, chunk_rows), chunk_rows)

    def copies(s, where):
        return (
            pltpu.make_async_copy(k_hbm.at[s, where], k_buf.at[s, where], k_sem.at[s]),
            pltpu.make_async_copy(v_hbm.at[s, where], v_buf.at[s, where], v_sem.at[s]),
        )

    def used(s):
        return (lens_ref[s] + chunk - 1) // chunk

    def fetch(s, _):
        n = used(s)
        for c in range(chunks):
            where = pl.ds(c * chunk_rows, chunk_rows)

            @pl.when(c < n)
            def _():
                for copy in copies(s, where):
                    copy.start()

            @pl.when(c >= n)
            def _():
                v_buf[s, where] = jnp.zeros((chunk_rows, width), v_buf.dtype)

        return 0

    lax.fori_loop(0, count, fetch, 0)

    member = member_ref[0]
    place = lax.broadcasted_iota(jnp.int32, (count, width), 1) // shard
    for h in range(heads):
        head = r_ref[h].astype(jnp.float32)
        bit = 1
        while bit * shard < width:
            turned = jnp.where(
                (place // bit) % 2 == 0,
                pltpu.roll(head, width - bit * shard, 1),
                pltpu.roll(head, bit * shard, 1),
            )
            head = jnp.where((member // bit) % 2 == 1, turned, head)
            bit *= 2
        q_buf[:, h, :] = head

    lane = lax.broadcasted_iota(jnp.int32, (heads, width), 1)
    head_row = lax.broadcasted_iota(jnp.int32, (heads, width), 0)
    column = lax.broadcasted_iota(jnp.int32, (1, heads, rows), 2)
    score_head = lax.broadcasted_iota(jnp.int32, (1, heads, rows), 1)
    own_kv = (column % kv_count) == score_head // group
    position = jnp.where(own_kv, column // kv_count, rows)[None]
    gain = gain_ref[...].astype(jnp.float32)
    lam = jnp.zeros((heads, 1), jnp.float32)
    for h in range(heads):
        lam = jnp.where(head_row[:, :1] == h, lam_ref[h], lam)
    lam = lam[None]
    low = (lane < half)[None]
    block = lax.broadcasted_iota(jnp.int32, (group_size, 1, heads, 1), 0)

    def spread(values):
        out = jnp.zeros((group_size, heads, width), jnp.float32)
        for k in range(kv_count):
            part = values[:, k * width : (k + 1) * width].reshape(group_size, 1, width)
            out = jnp.where((head_row // group == k)[None], part, out)
        return out

    def step(g, _):
        first = g * group_size
        here = pl.ds(first, group_size)
        q = q_buf[here].astype(jnp.bfloat16)
        zero = jnp.zeros_like(q)
        split = jnp.stack([jnp.where(low, q, zero), jnp.where(low, zero, q)], axis=1)
        own_key = spread(nk_ref[here].astype(jnp.float32))
        own_val = spread(nv_ref[here].astype(jnp.float32))
        own_score = (
            jnp.sum(split.astype(jnp.float32) * own_key[:, None], axis=3, keepdims=True) * inv_scale
        )
        limit = jnp.zeros((group_size, 1, heads, 1), jnp.int32)
        for i in range(group_size):
            s = first + i
            limit = jnp.where(block == i, lens_ref[s], limit)

            def wait(c, _):
                for copy in copies(s, piece(c)):
                    copy.wait()
                return 0

            lax.fori_loop(0, used(s), wait, 0)
        for i in range(group_size):
            s_buf[i] = lax.dot_general(
                split[i].reshape(2 * heads, width), k_buf[first + i], (((1,), (1,)), ((), ())), preferred_element_type=jnp.float32
            ).reshape(2, heads, rows)
        scores = jnp.where(position < limit, s_buf[...] * inv_scale, masked_score)
        highest = jnp.maximum(jnp.max(scores, axis=3, keepdims=True), own_score)
        expd = jnp.exp(scores - highest)
        own_exp = jnp.exp(own_score - highest)
        inverse = 1.0 / (jnp.sum(expd, axis=3, keepdims=True) + own_exp)
        plus = inverse[:, 0]
        minus = inverse[:, 1] * lam
        weights = (expd[:, 0] * plus - expd[:, 1] * minus).astype(jnp.bfloat16)
        own_weight = (own_exp[:, 0] * plus - own_exp[:, 1] * minus).astype(jnp.bfloat16)
        attended = jnp.stack(
            [
                jnp.dot(weights[i], v_buf[first + i], preferred_element_type=jnp.float32)
                for i in range(group_size)
            ]
        )
        attended = attended + own_weight.astype(jnp.float32) * own_val
        scale = lax.rsqrt(jnp.mean(attended * attended, axis=2, keepdims=True) + epsilon)
        q_buf[here] = (attended * scale * gain[None]).astype(o_ref.dtype).astype(jnp.float32)
        return 0

    lax.fori_loop(0, count // group_size, step, 0)
    heads_out = jnp.concatenate([q_buf[:, h, :] for h in range(heads)], axis=1).astype(o_ref.dtype)
    o_ref[...] = heads_out
    chosen = disp_ref[...]
    full = jnp.concatenate(
        [heads_out, jnp.zeros((chosen.shape[1] - count, heads * width), o_ref.dtype)], axis=0
    )
    put_rows(
        out_ref,
        pl.ds(0, heads * width),
        jnp.dot(chosen, full, preferred_element_type=jnp.float32).astype(out_ref.dtype),
    )


def attention(
    queries, new_keys, new_values, cache_keys, cache_values, lengths, lambdas, head_gain, dispatch, experts
):
    count, ctx_len, kv_count, width = cache_keys.shape
    heads = lambdas.shape[0]
    slots = dispatch.shape[0]
    shard = heads * width // experts
    vmem = pl.BlockSpec(memory_space=pltpu.VMEM)
    smem = pl.BlockSpec(memory_space=pltpu.SMEM)
    hbm = pl.BlockSpec(memory_space=pltpu.HBM)
    rows = ctx_len * kv_count
    together = 8
    return pl.pallas_call(
        functools.partial(attention_kernel, together, 128, shard),
        out_shape=(
            jax.ShapeDtypeStruct((count, heads * width), jnp.bfloat16),
            jax.ShapeDtypeStruct((experts, slots // experts, heads * width), jnp.bfloat16),
        ),
        in_specs=[smem, smem, smem, vmem, vmem, vmem, vmem, vmem, hbm, hbm],
        out_specs=(vmem, vmem),
        scratch_shapes=[
            pltpu.VMEM((count, rows, width), jnp.bfloat16),
            pltpu.VMEM((count, rows, width), jnp.bfloat16),
            pltpu.VMEM((together, 2, heads, rows), jnp.float32),
            pltpu.VMEM((count, heads, width), jnp.float32),
            pltpu.SemaphoreType.DMA((count,)),
            pltpu.SemaphoreType.DMA((count,)),
        ],
        compiler_params=pltpu.CompilerParams(vmem_limit_bytes=53 * 2**20),
        name="attention",
    )(
        lax.axis_index(NEAR).astype(jnp.int32).reshape(1),
        lengths,
        lambdas,
        queries,
        new_keys,
        new_values,
        head_gain.reshape(1, width),
        dispatch,
        cache_keys.reshape(count, rows, width),
        cache_values.reshape(count, rows, width),
    )


def expert_kernel(
    core_ref, h_ref, rows_ref, own_ref, tok_ref, gain_ref, near_hbm, other_hbm, gate_hbm, up_hbm, down_hbm,
    o_ref, res_ref, wo_buf, gate_buf, up_buf, down_buf, wo_sem, gate_sem, up_sem, down_sem,
):
    core = core_ref[0]
    cols = wo_buf.shape[1] // 2
    depth = wo_buf.shape[2]
    slots = h_ref.shape[0] * h_ref.shape[1]
    pieces = down_sem.shape[0]
    width = o_ref.shape[2]
    step = width // pieces

    wo_copies = []
    for i, source in enumerate((near_hbm, other_hbm)):
        side = core if i == 0 else 1 - core
        at = pl.ds(pl.multiple_of(side * cols, cols), cols)
        wo_copies.append(
            pltpu.make_async_copy(source.at[:, pl.ds(0, cols)], wo_buf.at[:, at], wo_sem.at[i])
        )
    gate_copy = pltpu.make_async_copy(gate_hbm.at[0], gate_buf, gate_sem)
    up_copy = pltpu.make_async_copy(up_hbm.at[0], up_buf, up_sem)
    down_copies = [
        pltpu.make_async_copy(
            down_hbm.at[0, :, pl.ds(i * step, step)], down_buf.at[:, pl.ds(i * step, step)], down_sem.at[i]
        )
        for i in range(pieces)
    ]
    for copy in (*wo_copies, gate_copy, up_copy, *down_copies):
        copy.start()

    heads = jnp.concatenate([rows_of(h_ref), own_ref[...]], axis=0)
    for copy in wo_copies:
        copy.wait()
    attn = lax.dot_general(
        heads,
        wo_buf[...].reshape(width, depth),
        (((1,), (1,)), ((), ())),
        preferred_element_type=jnp.float32,
    ).astype(jnp.bfloat16)
    res_ref[...] = (
        tok_ref[...].astype(jnp.float32) + attn[slots:].astype(jnp.float32)
    ).astype(res_ref.dtype)
    residual = (
        rows_ref[...].astype(jnp.float32) + attn[:slots].astype(jnp.float32)
    ).astype(jnp.bfloat16)
    inputs = rms_scaled(residual, gain_ref[...]).astype(jnp.bfloat16)
    gate_copy.wait()
    gate = jnp.dot(inputs, gate_buf[...], preferred_element_type=jnp.float32)
    gate = jnp.minimum(gate, clamp_limit)
    swish = gate * (1.0 / (1.0 + jnp.exp(-swish_alpha * gate)))
    up_copy.wait()
    upper = jnp.dot(inputs, up_buf[...], preferred_element_type=jnp.float32)
    upper = jnp.clip(upper, -clamp_limit, clamp_limit)
    act = ((upper + 1.0) * swish).astype(jnp.bfloat16)
    for i, copy in enumerate(down_copies):
        copy.wait()
        at = pl.ds(i * step, step)
        put_rows(
            o_ref,
            at,
            jnp.dot(act, down_buf[:, at], preferred_element_type=jnp.float32).astype(o_ref.dtype),
        )


def expert(core, received, rows, head_out, tokens, moe_gain, near, other, cols, gate_w, up_w, down_w):
    members, per, _ = received.shape
    count, width = tokens.shape
    chips, _, depth = near.shape
    hidden = gate_w.shape[2]
    pieces = 4
    vmem = pl.BlockSpec(memory_space=pltpu.VMEM)
    smem = pl.BlockSpec(memory_space=pltpu.SMEM)
    hbm = pl.BlockSpec(memory_space=pltpu.HBM)
    bf16 = jnp.bfloat16
    return pl.pallas_call(
        expert_kernel,
        out_shape=(
            jax.ShapeDtypeStruct((members, per, width), bf16),
            jax.ShapeDtypeStruct((count, width), bf16),
        ),
        in_specs=[smem, vmem, vmem, vmem, vmem, vmem, hbm, hbm, hbm, hbm, hbm],
        out_specs=(vmem, vmem),
        scratch_shapes=[
            pltpu.VMEM((chips, 2 * cols, depth), bf16),
            pltpu.VMEM((width, hidden), bf16),
            pltpu.VMEM((width, hidden), bf16),
            pltpu.VMEM((hidden, width), bf16),
            pltpu.SemaphoreType.DMA((2,)),
            pltpu.SemaphoreType.DMA,
            pltpu.SemaphoreType.DMA,
            pltpu.SemaphoreType.DMA((pieces,)),
        ],
        compiler_params=pltpu.CompilerParams(vmem_limit_bytes=50 * 2**20),
        name="expert",
    )(core, received, rows, head_out, tokens, moe_gain.reshape(1, width), near, other, gate_w, up_w, down_w)


def pick_kernel(cols, count, where_ref, near_hbm, other_hbm, o_ref, x_buf, name_buf, x_sem, name_sem):
    core = where_ref[0]
    expert = where_ref[1].astype(jnp.float32)
    halves, chips, _, depth = x_buf.shape
    names = name_buf.shape[1] // 2
    lanes = name_buf.shape[2]
    members = 2 * chips
    slots = o_ref.shape[0]
    per = slots // members
    copies = []
    for i, source in enumerate((near_hbm, other_hbm)):
        side = core if i == 0 else 1 - core
        at = pl.ds(pl.multiple_of(side * names, names), names)
        first = cols + halves * count
        copies.append(
            pltpu.make_async_copy(
                source.at[:, pl.ds(first, names), pl.ds(0, lanes)], name_buf.at[:, at], name_sem.at[i]
            )
        )
    for i, source in enumerate((near_hbm, other_hbm)):
        side = core if i == 0 else 1 - core
        at = pl.ds(pl.multiple_of(side * count, count), count)
        for half in range(halves):
            rows = pl.ds(cols + half * count, count)
            copies.append(
                pltpu.make_async_copy(
                    source.at[:, rows], x_buf.at[half, :, at], x_sem.at[i * halves + half]
                )
            )
    for copy in copies:
        copy.start()

    def table(shape, rule):
        rows = lax.broadcasted_iota(jnp.int32, shape, 0)
        columns = lax.broadcasted_iota(jnp.int32, shape, 1)
        return jnp.where(rule(rows, columns), 1.0, 0.0).astype(jnp.bfloat16)

    def product(a, b):
        return jnp.dot(a, b, preferred_element_type=jnp.float32)

    for copy in copies[:2]:
        copy.wait()
    named = name_buf[...].reshape(members * names, lanes).astype(jnp.float32)
    found = jnp.where(named == expert, 1.0, 0.0).astype(jnp.bfloat16)
    found = product(table((members, members * names), lambda r, c: c // names == r), found)
    found = found.astype(jnp.bfloat16)
    earlier = product(found, table((lanes, lanes), lambda r, c: r < c)).astype(jnp.bfloat16)
    repeat = table((slots, members), lambda r, c: r // per == c)
    rank = lax.broadcasted_iota(jnp.int32, (slots, lanes), 0) % per
    chosen = jnp.where(
        product(repeat, earlier) == rank.astype(jnp.float32), product(repeat, found), 0.0
    ).astype(jnp.bfloat16)
    spread = product(chosen, table((lanes, members * count), lambda r, c: c % count == r))
    slot = lax.broadcasted_iota(jnp.int32, (slots, members * count), 0)
    column = lax.broadcasted_iota(jnp.int32, (slots, members * count), 1)
    select = jnp.where(slot // per == column // count, spread, 0.0).astype(jnp.bfloat16)
    for copy in copies[2:]:
        copy.wait()
    for half in range(halves):
        o_ref[:, pl.ds(half * depth, depth)] = product(
            select, x_buf[half].reshape(members * count, depth)
        ).astype(o_ref.dtype)


def pick(where, near, other, cols, slots, tokens):
    count, width = tokens.shape
    chips, packed, depth = near.shape
    halves = width // depth
    names = packed - cols - halves * count
    hbm = pl.BlockSpec(memory_space=pltpu.HBM)
    return pl.pallas_call(
        functools.partial(pick_kernel, cols, count),
        out_shape=jax.ShapeDtypeStruct((slots, width), jnp.bfloat16),
        in_specs=[pl.BlockSpec(memory_space=pltpu.SMEM), hbm, hbm],
        out_specs=pl.BlockSpec(memory_space=pltpu.VMEM),
        scratch_shapes=[
            pltpu.VMEM((halves, chips, 2 * count, depth), jnp.bfloat16),
            pltpu.VMEM((chips, 2 * names, 128), jnp.bfloat16),
            pltpu.SemaphoreType.DMA((2 * halves,)),
            pltpu.SemaphoreType.DMA((2,)),
        ],
        compiler_params=pltpu.CompilerParams(vmem_limit_bytes=50 * 2**20),
        name="pick",
    )(where, near, other)


def combine_kernel(share_ref, rows_ref, res_ref, o_ref):
    share = share_ref[...]
    high = share.astype(jnp.bfloat16)
    low = (share - high.astype(jnp.float32)).astype(jnp.bfloat16)
    rows = rows_of(rows_ref)
    total = jnp.dot(high, rows, preferred_element_type=jnp.float32) + jnp.dot(
        low, rows, preferred_element_type=jnp.float32
    )
    o_ref[...] = (res_ref[...].astype(jnp.float32) + total).astype(o_ref.dtype)


def combine(share, rows, residual):
    vmem = pl.BlockSpec(memory_space=pltpu.VMEM)
    return pl.pallas_call(
        combine_kernel,
        out_shape=jax.ShapeDtypeStruct(residual.shape, jnp.bfloat16),
        in_specs=[vmem] * 3,
        out_specs=vmem,
        compiler_params=pltpu.CompilerParams(vmem_limit_bytes=32 * 2**20),
        name="combine",
    )(share, rows, residual)


def local(
    tokens,
    norm_gain,
    query_weight,
    key_weight,
    value_weight,
    out_weight,
    head_gain,
    lambdas,
    cache_keys,
    cache_values,
    lengths,
    moe_gain,
    gate_weight,
    up_weight,
    down_weight,
    routes,
    route_weights,
):
    count = tokens.shape[0]
    topk = routes.shape[1]
    packed = pack(out_weight, tokens, routes)
    near_packed = lax.all_gather(packed, CHIPS, axis=0)
    part, normed = query_product(tokens, norm_gain, query_weight)
    queries = lax.all_to_all(part, "far", 0, 0, tiled=True)
    new_keys = jnp.dot(normed, key_weight, preferred_element_type=jnp.float32).astype(jnp.bfloat16)
    new_values = jnp.dot(normed, value_weight, preferred_element_type=jnp.float32).astype(
        jnp.bfloat16
    )
    experts = lax.axis_size(EP)
    capacity = min(count, max(2, 2 * count * topk // experts))
    routes, new_keys = lax.optimization_barrier((routes, new_keys))
    slot_range = jnp.arange(experts * capacity, dtype=jnp.int32)
    onehot = (
        routes.reshape(-1)[:, None] == jnp.arange(experts, dtype=jnp.int32)[None, :]
    ).astype(jnp.int32)
    earlier_all = jnp.cumsum(onehot, axis=0) - onehot
    ranks = jnp.sum(earlier_all * onehot, axis=1).reshape(count, topk)
    slot_id = routes * capacity + ranks
    dispatch = jnp.any(slot_id[None, :, :] == slot_range[:, None, None], axis=2).astype(
        jnp.bfloat16
    )
    dispatch = jnp.pad(dispatch, ((0, 0), (0, 128 - count)))
    share = jnp.sum(
        jnp.where(slot_id[:, :, None] == slot_range[None, None, :], route_weights[:, :, None], 0.0),
        axis=1,
    )
    head_out, outgoing = attention(
        queries, new_keys, new_values, cache_keys, cache_values, lengths, lambdas, head_gain, dispatch, experts
    )
    received = lax.all_to_all(outgoing, EP, split_axis=0, concat_axis=0, tiled=True)
    near_packed, head_out = lax.optimization_barrier((near_packed, head_out))
    other_packed = lax.ppermute(near_packed, "core", [(0, 1), (1, 0)])
    core = lax.axis_index("core").astype(jnp.int32)
    where = jnp.stack([core, lax.axis_index(EP).astype(jnp.int32)])
    cols = out_weight.shape[1]
    rows = pick(where, near_packed, other_packed, cols, experts * capacity, tokens)
    results, residual = expert(
        where,
        received,
        rows,
        head_out,
        tokens,
        moe_gain,
        near_packed,
        other_packed,
        cols,
        gate_weight,
        up_weight,
        down_weight,
    )
    returned = lax.all_to_all(results, EP, split_axis=0, concat_axis=0, tiled=True)
    return combine(share, returned, residual)


def solution(mesh):
    devices = mesh.devices.reshape(mesh.shape["grp"], -1, 2, 2)
    torus = Mesh(devices, ("grp", "far", "near", "core"))
    return jax.shard_map(
        local,
        mesh=torus,
        in_specs=(
            P(GRP_EP, None),
            P(),
            P(None, EP),
            P(),
            P(),
            P(None, EP),
            P(),
            P(),
            P(GRP_EP, None, None, None),
            P(GRP_EP, None, None, None),
            P(GRP_EP),
            P(),
            P(EP, None, None),
            P(EP, None, None),
            P(EP, None, None),
            P(GRP_EP, None),
            P(GRP_EP, None),
        ),
        out_specs=P(GRP_EP, None),
        check_vma=False,
    )
```
